512 devices in a mesh: sp: 64 (over z, y), fs: 4 (over x), tp: 2 (over core).
Axes of the slice: x: 4, y: 8, z: 8, core: 2. Of those that a mesh axis runs over, the one named last changes fastest.
Arguments:
- activations: bfloat16 [4, 16384, 2048], P('fs', 'sp'), may hold values from -600 to 600
- norm_gain: float32 [2048], replicated, may hold values from 0.1 to 1.9
- w_conv_gate: bfloat16 [2048, 1024], P('sp', ('fs', 'tp')), may hold values from -0.125 to 0.125
- w_conv_mult: bfloat16 [2048, 1024], P('sp', ('fs', 'tp')), may hold values from -0.125 to 0.125
- w_conv_in: bfloat16 [2048, 1024], P('sp', ('fs', 'tp')), may hold values from -0.125 to 0.125
- conv_taps: float32 [3, 1024], replicated, may hold values from -3.5 to 3.5
- w_query: bfloat16 [2048, 1024], P('sp', ('fs', 'tp')), may hold values from -0.125 to 0.125
- w_key: bfloat16 [2048, 1024], P('sp', ('fs', 'tp')), may hold values from -0.125 to 0.125
- w_value: bfloat16 [2048, 1024], P('sp', ('fs', 'tp')), may hold values from -0.125 to 0.125
- w_input_gate: bfloat16 [2048, 8], replicated, may hold values from -0.125 to 0.125
- w_forget_gate: bfloat16 [2048, 8], replicated, may hold values from -0.125 to 0.125
- gate_bias: float32 [2, 8], replicated, may hold values from -1 to 120
- decay_shift: float32 [4, 16384, 8], P(None, 'sp'), may hold values from -2 to 0, as said below
- head_gain: float32 [1024], replicated, may hold values from 0.1 to 1.9
- w_out_conv: bfloat16 [1024, 2048], P(('fs', 'tp'), 'sp'), may hold values from -0.125 to 0.125
- w_out_mem: bfloat16 [1024, 2048], P(('fs', 'tp'), 'sp'), may hold values from -0.125 to 0.125
Outputs:
- output: bfloat16 [4, 16384, 2048], P('fs', ('sp', 'tp'))
The draws below stay inside these ranges and needn't reach their ends.
Inputs may be any that keep to these rules, and one draw needn't show every extreme that they name: `decay_shift`: never positive.
All inputs are finite; a program needn't handle non-finite values.
Results may differ from the reference program's by a relative error of at most 0.015.
Values may be sent and summed in bfloat16 or wider, within the bound.
No kernel may reach another device: no remote copies, remote signals or barrier semaphores. Data moves between devices by JAX's collectives and lax.ppermute only.
A program may use at most 64 MiB of HBM per device.

```python
import math
import jax
import jax.numpy as jnp
from jax import lax

D = 2048
CONV_CH = 1024
MEMORY_HEADS = 8
HEAD_DIM = 128
BLOCK = 64
TAPS = 3
TOK_DEV = 256
SEQUENCE_COUNT = 4
SEQUENCE_LENGTH = 16384


def draw_activations(key, part):
    random_subkeys = jax.random.split(key, 3)
    row_scale = jnp.exp(jax.random.uniform(random_subkeys[0], (SEQUENCE_COUNT, SEQUENCE_LENGTH, 1), jnp.float32, 0.0, math.log(10.0)))
    col_scale = jnp.exp(jax.random.uniform(random_subkeys[1], (1, 1, D), jnp.float32, 0.0, math.log(10.0)))
    base_values = jnp.clip(jax.random.normal(random_subkeys[2], (SEQUENCE_COUNT, SEQUENCE_LENGTH, D), jnp.float32), -6.0, 6.0)
    return (base_values * row_scale * col_scale).astype(jnp.bfloat16)


def draw_gate_bias(key, part):
    random_subkeys = jax.random.split(key, 4)
    ranking = jax.random.permutation(random_subkeys[0], MEMORY_HEADS)
    slow_heads = ranking < MEMORY_HEADS // 2
    entry_bias = jax.random.uniform(random_subkeys[1], (MEMORY_HEADS,), jnp.float32, -1.0, 1.0)
    slow_bias = math.log(SEQUENCE_LENGTH) + 2.0 + jax.random.uniform(random_subkeys[2], (MEMORY_HEADS,), jnp.float32, -0.3, 0.3)
    fast_bias = jax.random.uniform(random_subkeys[3], (MEMORY_HEADS,), jnp.float32, 3.0, 4.5)
    forget = jnp.where(slow_heads, slow_bias, fast_bias)
    return jnp.stack([entry_bias, forget], axis=0)


def draw_decay_shift(key, part):
    random_subkeys = jax.random.split(key, 3)
    nblocks = SEQUENCE_LENGTH // TOK_DEV
    low_rate, high_rate = (0.2, 2.0)
    rates = jnp.exp(jax.random.uniform(random_subkeys[0], (SEQUENCE_COUNT, nblocks, 1, MEMORY_HEADS), jnp.float32, math.log(low_rate), math.log(high_rate)))
    stable_part = -jnp.broadcast_to(rates, (SEQUENCE_COUNT, nblocks, TOK_DEV, MEMORY_HEADS)).reshape(SEQUENCE_COUNT, SEQUENCE_LENGTH, MEMORY_HEADS) / SEQUENCE_LENGTH
    spike_positions = jax.random.randint(random_subkeys[1], (SEQUENCE_COUNT, 2, MEMORY_HEADS), 0, SEQUENCE_LENGTH)
    spike_penalty = jax.random.uniform(random_subkeys[2], (SEQUENCE_COUNT, 2, MEMORY_HEADS), jnp.float32, 0.2, 0.5)
    chosen_positions = jnp.arange(SEQUENCE_LENGTH)[None, :, None, None]
    match_count = (chosen_positions == spike_positions[:, None, :, :]).astype(jnp.float32)
    spike_events = jnp.sum(match_count * jnp.log(1.0 - spike_penalty)[:, None, :, :], axis=2)
    return stable_part + spike_events


def steps_of(stream_key, shape, cuts, least, largest):
    gain, own = 1.0, jax.random.fold_in(stream_key, 6)
    for axis_at, parts in cuts:
        steps = jnp.exp(jax.random.uniform(jax.random.fold_in(own, axis_at), (parts,), jnp.float32, least / len(cuts), largest / len(cuts)))
        gain = gain * jnp.repeat(steps, shape[axis_at] // parts).reshape([-1 if axis == axis_at else 1 for axis in range(len(shape))])
    return gain


def gaussian(rng, dims, deviation, bound, cuts=(), held_as=jnp.bfloat16):
    entries = jax.random.normal(rng, dims, jnp.float32) * deviation
    if len(cuts) > 0:
        entries = steps_of(rng, dims, cuts, -0.22, 0.18) * entries
    return jnp.clip(entries, min=-bound, max=bound).astype(held_as)


def setup_inputs(seed: int = 0) -> dict:
    splits = jax.random.split(jax.random.key(seed), 17)
    return {
        "activations": draw_activations(jax.random.fold_in(splits[16], 71), 0),
        "norm_gain": jnp.clip(1.0 + 0.18 * jax.random.normal(splits[1], (D,), jnp.float32), 0.1, 1.9),
        "w_conv_gate": gaussian(splits[2], (D, CONV_CH), D ** -0.5, 0.125, ((0, 64), (1, 8))),
        "w_conv_mult": gaussian(splits[3], (D, CONV_CH), D ** -0.5, 0.125, ((0, 64), (1, 8))),
        "w_conv_in": gaussian(splits[4], (D, CONV_CH), D ** -0.5, 0.125, ((0, 64), (1, 8))),
        "conv_taps": gaussian(splits[5], (TAPS, CONV_CH), TAPS ** -0.5, 3.5, (), jnp.float32),
        "w_query": gaussian(splits[6], (D, MEMORY_HEADS * HEAD_DIM), D ** -0.5, 0.125, ((0, 64), (1, 8))),
        "w_key": gaussian(splits[7], (D, MEMORY_HEADS * HEAD_DIM), D ** -0.5, 0.125, ((0, 64), (1, 8))),
        "w_value": gaussian(splits[8], (D, MEMORY_HEADS * HEAD_DIM), D ** -0.5, 0.125, ((0, 64), (1, 8))),
        "w_input_gate": gaussian(splits[9], (D, MEMORY_HEADS), D ** -0.5, 0.125),
        "w_forget_gate": gaussian(splits[10], (D, MEMORY_HEADS), D ** -0.5, 0.125),
        "gate_bias": draw_gate_bias(jax.random.fold_in(splits[16], 71), 0),
        "decay_shift": draw_decay_shift(jax.random.fold_in(splits[16], 71), 0),
        "head_gain": jnp.clip(1.0 + 0.18 * jax.random.normal(splits[13], (MEMORY_HEADS * HEAD_DIM,), jnp.float32), 0.1, 1.9),
        "w_out_conv": gaussian(splits[14], (CONV_CH, D), (CONV_CH + MEMORY_HEADS * HEAD_DIM) ** -0.5, 0.125, ((0, 8), (1, 64))),
        "w_out_mem": gaussian(splits[15], (MEMORY_HEADS * HEAD_DIM, D), (CONV_CH + MEMORY_HEADS * HEAD_DIM) ** -0.5, 0.125, ((0, 8), (1, 64))),
    }


EPSILON = 1e-06
HIGHEST_PRECISION = lax.Precision.HIGHEST

def combine_states(earlier, later):
    total_one, peak_one, state_one = earlier
    total_two, peak_two, state_two = later
    peak_new = jnp.maximum(total_two + peak_one, peak_two)
    scale_old = jnp.exp(total_two + peak_one - peak_new)
    scale_new = jnp.exp(peak_two - peak_new)
    return (total_one + total_two, peak_new, scale_old[..., None, None] * state_one + scale_new[..., None, None] * state_two)

def head_memory(block_inputs):
    query_rows, key_rows, value_rows, entry_gate, log_forget = block_inputs
    members = query_rows.shape[0]
    tokens = query_rows.shape[1]
    head_width = query_rows.shape[2]
    nblocks = tokens // BLOCK
    block_shape = (members, nblocks, BLOCK, head_width)
    query_blocks = query_rows.astype(jnp.float32).reshape(block_shape)
    key_blocks = key_rows.astype(jnp.float32).reshape(block_shape) * head_width ** (-0.5)
    value_blocks = value_rows.astype(jnp.float32).reshape(block_shape)
    entry_blocks = entry_gate.reshape(members, nblocks, BLOCK)
    forget_sums = jnp.cumsum(log_forget.reshape(members, nblocks, BLOCK), axis=-1)
    block_total = forget_sums[..., -1]
    local_logs = block_total[..., None] - forget_sums + entry_blocks
    local_peak = lax.optimization_barrier(jnp.max(local_logs, axis=-1))
    local_weights = jnp.exp(local_logs - local_peak[..., None])
    local_state = jnp.einsum('bclv,bclk->bcvk', local_weights[..., None] * value_blocks, key_blocks, precision=HIGHEST_PRECISION)

    def advance(running, block_item):
        return (combine_states(running, block_item), running)
    anchor = (jnp.zeros((members,), jnp.float32), jnp.zeros((members,), jnp.float32), jnp.zeros((members, head_width, head_width), jnp.float32))
    block_items = (jnp.moveaxis(block_total, 1, 0), jnp.moveaxis(local_peak, 1, 0), jnp.moveaxis(local_state, 1, 0))
    _, prior_states = lax.scan(advance, anchor, block_items)
    prior_peak = jnp.moveaxis(prior_states[1], 0, 1)
    prior_state = jnp.moveaxis(prior_states[2], 0, 1)
    positions = jnp.arange(BLOCK)
    causal_mask = positions[:, None] >= positions[None, :]
    pair_logs = jnp.where(causal_mask, forget_sums[..., :, None] - forget_sums[..., None, :] + entry_blocks[..., None, :], -jnp.inf)
    carried_logs = forget_sums + prior_peak[..., None]
    row_peak = jnp.maximum(carried_logs, lax.optimization_barrier(jnp.max(pair_logs, axis=-1)))
    inner_weights = jnp.exp(pair_logs - row_peak[..., None])
    carried_weights = jnp.exp(carried_logs - row_peak)
    scores = inner_weights * jnp.einsum('bcld,bcsd->bcls', query_blocks, key_blocks, precision=HIGHEST_PRECISION)
    numerator = carried_weights[..., None] * jnp.einsum('bcvk,bclk->bclv', prior_state, query_blocks, precision=HIGHEST_PRECISION) + jnp.einsum('bcls,bcsv->bclv', scores, value_blocks, precision=HIGHEST_PRECISION)
    return numerator.reshape(members, tokens, head_width)

def reference(activations, norm_gain, w_conv_gate, w_conv_mult, w_conv_in, conv_taps, w_query, w_key, w_value, w_input_gate, w_forget_gate, gate_bias, decay_shift, head_gain, w_out_conv, w_out_mem):
    seq_count = activations.shape[0]
    length = activations.shape[1]
    model_width = activations.shape[2]
    flat_rows = activations.reshape(seq_count * length, model_width).astype(jnp.float32)
    normed = (flat_rows * lax.rsqrt(lax.optimization_barrier(jnp.mean(flat_rows * flat_rows, axis=-1, keepdims=True)) + EPSILON) * norm_gain).astype(jnp.bfloat16)

    def project(weight):
        return jnp.dot(normed, weight, preferred_element_type=jnp.float32).astype(jnp.bfloat16)
    conv_gate = project(w_conv_gate).reshape(seq_count, length, CONV_CH)
    conv_mult = project(w_conv_mult).reshape(seq_count, length, CONV_CH)
    conv_in = project(w_conv_in).reshape(seq_count, length, CONV_CH)
    product = (conv_mult.astype(jnp.float32) * conv_in.astype(jnp.float32)).astype(jnp.bfloat16)
    padded = jnp.pad(product, ((0, 0), (TAPS - 1, 0), (0, 0))).astype(jnp.float32)
    mixed_sum = jnp.zeros((seq_count, length, CONV_CH), jnp.float32)
    for tap_index in range(TAPS):
        mixed_sum = mixed_sum + conv_taps[tap_index] * padded[:, tap_index:tap_index + length, :]
    conv_out = (conv_gate.astype(jnp.float32) * mixed_sum).astype(jnp.bfloat16)

    def heads_first(values, inner):
        return jnp.moveaxis(values.reshape(seq_count, length, MEMORY_HEADS, inner), 2, 0)
    query_heads = heads_first(project(w_query), HEAD_DIM)
    key_heads = heads_first(project(w_key), HEAD_DIM)
    value_heads = heads_first(project(w_value), HEAD_DIM)
    entry = jnp.dot(normed, w_input_gate, preferred_element_type=jnp.float32) + gate_bias[0]
    log_forget = jax.nn.log_sigmoid(jnp.dot(normed, w_forget_gate, preferred_element_type=jnp.float32) + gate_bias[1]) + decay_shift.reshape(seq_count * length, MEMORY_HEADS)
    entry_heads = jnp.moveaxis(entry.reshape(seq_count, length, MEMORY_HEADS), 2, 0)
    forget_heads = jnp.moveaxis(log_forget.reshape(seq_count, length, MEMORY_HEADS), 2, 0)
    memory = lax.map(head_memory, (query_heads, key_heads, value_heads, entry_heads, forget_heads))
    memory = memory * lax.rsqrt(lax.optimization_barrier(jnp.mean(memory * memory, axis=-1, keepdims=True)) + EPSILON) * head_gain.reshape(MEMORY_HEADS, 1, 1, HEAD_DIM)
    mem_out = jnp.moveaxis(memory, 0, 2).reshape(seq_count * length, MEMORY_HEADS * HEAD_DIM).astype(jnp.bfloat16)
    output = jnp.dot(conv_out.reshape(seq_count * length, CONV_CH), w_out_conv, preferred_element_type=jnp.float32) + jnp.dot(mem_out, w_out_mem, preferred_element_type=jnp.float32)
    return output.astype(jnp.bfloat16).reshape(seq_count, length, model_width)
```

```python
import jax
import jax.numpy as jnp
from jax import lax
from jax.experimental import pallas as pl
from jax.experimental.pallas import tpu as pltpu
from jax.sharding import Mesh
from jax.sharding import PartitionSpec as P


HEAD_DIM = 128
SP = ("sp_0", "sp_1")
SP_TP = ("sp_0", "sp_1", "tp")
EPSILON = 1e-06
HIGHEST = lax.Precision.HIGHEST
F32 = jnp.float32
BF16 = jnp.bfloat16


def everyone(array, axis):
    copies = jnp.broadcast_to(array, (lax.axis_size(axis), *array.shape))
    return lax.all_to_all(copies, axis, split_axis=0, concat_axis=0, tiled=True)


def exchanged(array, axis):
    return lax.all_to_all(array, axis, split_axis=0, concat_axis=0, tiled=True)


def other_core(array):
    return lax.ppermute(array, "tp", [(0, 1), (1, 0)])


def from_behind(array, axis):
    peers = lax.axis_size(axis)
    return lax.ppermute(array, axis, [(i, i + 1) for i in range(peers - 1)])


def thirds(x):
    first = lax.reduce_precision(x, 8, 7)
    second = lax.reduce_precision(x - first, 8, 7)
    third = lax.reduce_precision(x - first - second, 8, 7)
    return jnp.stack([first, second, third])


def dot(a, b, dims):
    return lax.dot_general(a, b, dims, preferred_element_type=F32)


def ring(array, axis, by):
    peers = lax.axis_size(axis)
    return lax.ppermute(array, axis, [(i, (i + by) % peers) for i in range(peers)])


def around(array, axis):
    behind = ring(array, axis, 1)
    ahead = ring(array, axis, -1)
    cut = array.shape[0] // 2
    far = jnp.concatenate(
        [ring(behind[:cut], axis, 1), ring(ahead[cut:], axis, -1)], axis=0
    )
    return behind, ahead, far


def returned(blocks, axis):
    own, behind, ahead, far = blocks
    return own, ring(ahead, axis, 1), ring(behind, axis, -1), ring(far, axis, 2)


def project_kernel(core, *refs):
    pieces, weights, gate_rows, out, gates = refs[:8], refs[8], refs[9], refs[10], refs[11]
    half = pieces[0].shape[1]
    first = pl.multiple_of(core[0] * half, half)
    second = pl.multiple_of((1 - core[0]) * half, half)
    for k in range(4):
        a, b = pieces[2 * k][...], pieces[2 * k + 1][...]
        mixed = jnp.dot(a, weights[pl.ds(first, half), :], preferred_element_type=F32)
        mixed += jnp.dot(b, weights[pl.ds(second, half), :], preferred_element_type=F32)
        out[k] = mixed.astype(BF16)
        dims = (((1,), (1,)), ((), ()))
        rows = dot(gate_rows[core[0]], a, dims)
        gates[k] = rows + dot(gate_rows[1 - core[0]], b, dims)


def project_only_kernel(core, *refs):
    pieces, weights, out = refs[:8], refs[8], refs[9]
    half = pieces[0].shape[1]
    first = pl.multiple_of(core[0] * half, half)
    second = pl.multiple_of((1 - core[0]) * half, half)
    for k in range(4):
        mixed = jnp.dot(
            pieces[2 * k][...], weights[pl.ds(first, half), :], preferred_element_type=F32
        )
        mixed += jnp.dot(
            pieces[2 * k + 1][...], weights[pl.ds(second, half), :], preferred_element_type=F32
        )
        out[k] = mixed.astype(BF16)


def in_vmem(count):
    return [pl.BlockSpec(memory_space=pltpu.VMEM)] * count


def project(core, pieces, weights, gate_rows=None):
    tokens = pieces[0].shape[0]
    shape = jax.ShapeDtypeStruct((4, tokens, weights.shape[1]), BF16)
    smem = [pl.BlockSpec(memory_space=pltpu.SMEM)]
    flops = 8 * tokens * weights.size
    cost = pl.CostEstimate(flops=flops, bytes_accessed=6 << 20, transcendentals=0)
    if gate_rows is None:
        return pl.pallas_call(
            project_only_kernel,
            out_shape=shape,
            in_specs=smem + in_vmem(9),
            out_specs=in_vmem(1)[0],
            cost_estimate=cost,
        )(core, *pieces, weights)
    return pl.pallas_call(
        project_kernel,
        out_shape=(shape, jax.ShapeDtypeStruct((4, gate_rows.shape[1], tokens), F32)),
        in_specs=smem + in_vmem(10),
        out_specs=in_vmem(2),
        cost_estimate=cost,
    )(core, *pieces, weights, gate_rows)


def shards(
    activations,
    norm_gain,
    w_conv_gate,
    w_conv_mult,
    w_conv_in,
    conv_taps,
    w_query,
    w_key,
    w_value,
    w_input_gate,
    w_forget_gate,
    gate_bias,
    decay_shift,
    head_gain,
    w_out_conv,
    w_out_mem,
):
    head = lax.axis_index("fs") * lax.axis_size("tp") + lax.axis_index("tp")
    core = lax.axis_index("tp")
    tokens, width = activations.shape[1:]
    half = width // 2
    seqs = lax.axis_size("fs")

    place_x = lax.axis_index("fs")
    order = [(place_x + by) % seqs for by in (0, seqs - 1, 1, 2)]

    w_conv = jnp.concatenate([w_conv_gate, w_conv_mult, w_conv_in], axis=1)
    w_conv = lax.all_gather(w_conv, SP, axis=0, tiled=True)
    w_mem = everyone(jnp.concatenate([w_query, w_key, w_value], axis=1), SP)
    w_mem = w_mem.reshape(width, -1)

    turned = jnp.concatenate([w_out_conv.T, w_out_mem.T], axis=1)
    turned, w_mem = lax.optimization_barrier((turned, w_mem))
    w_own = everyone(turned, SP).reshape(width, -1)
    w_out = (w_own, *around(w_own, "fs"))

    x = activations[0].astype(F32)
    normed = (
        x * lax.rsqrt(jnp.mean(x * x, axis=-1, keepdims=True) + EPSILON) * norm_gain
    ).astype(BF16)
    mine = lax.dynamic_slice_in_dim(normed, core * half, half, 1)
    pieces = [mine, lax.dynamic_slice_in_dim(normed, (1 - core) * half, half, 1)]
    for piece in around(mine, "fs"):
        pieces += [piece, other_core(piece)]
    core_row = core.reshape(1).astype(jnp.int32)

    gate_rows = jnp.concatenate(
        [
            lax.dynamic_slice_in_dim(w_input_gate, head, 1, 1),
            lax.dynamic_slice_in_dim(w_forget_gate, head, 1, 1),
        ],
        axis=1,
    ).T
    gate_rows = jnp.pad(gate_rows, ((0, 14), (0, 0))).reshape(16, 2, half).transpose(1, 0, 2)
    qkv, gates = project(core_row, pieces, w_mem, gate_rows)
    query, key, value = (qkv[..., k * HEAD_DIM : (k + 1) * HEAD_DIM] for k in range(3))
    bias = lax.dynamic_slice_in_dim(gate_bias, head, 1, 1)
    decay = lax.dynamic_slice_in_dim(decay_shift, head, 1, 2)[..., 0]
    decay = jnp.concatenate([lax.dynamic_slice_in_dim(decay, k, 1, 0) for k in order], axis=0)
    entry = gates[:, 0] + bias[0]
    log_forget = jax.nn.log_sigmoid(gates[:, 1] + bias[1]) + decay
    sums = jnp.cumsum(log_forget, axis=-1)
    total = sums[:, -1]
    local_logs = total[:, None] - sums + entry
    peak = jnp.max(local_logs, axis=-1)
    scale = HEAD_DIM ** (-0.5)
    local_weights = jnp.exp(local_logs - peak[:, None]) * scale

    weighted = (local_weights[..., None] * value.astype(F32)).astype(BF16)
    state = dot(weighted, key, (((1,), (1,)), ((0,), (0,))))

    places = lax.axis_size(SP)
    cut = HEAD_DIM // places
    slices = state.astype(BF16).reshape(seqs, places, cut, HEAD_DIM).transpose(1, 0, 2, 3)
    slices = slices.reshape(places, seqs * cut, HEAD_DIM)
    numbers = thirds(jnp.stack([total, peak])).astype(BF16).reshape(1, 1, -1)
    count = numbers.shape[2]
    numbers = jnp.pad(numbers, ((0, 0), (0, seqs * cut - 1), (0, HEAD_DIM - count)))
    numbers = jnp.broadcast_to(numbers, slices.shape)
    packed = jnp.concatenate([slices, numbers], axis=1)
    everywhere = exchanged(packed, SP)
    found = everywhere[:, seqs * cut, :count].astype(F32).reshape(places, 3, 2, seqs)
    found = found[:, 0] + found[:, 1] + found[:, 2]
    totals, peaks = found[:, 0].T, found[:, 1].T
    spots = jnp.arange(places)
    earlier = spots[:, None] > spots[None, :]
    masked = jnp.where(earlier, totals[:, None, :], 0.0)
    between = lax.dot_general(
        masked, earlier.astype(F32), (((2,), (0,)), ((), ())), precision=HIGHEST
    )
    since_start = jnp.sum(masked, axis=-1)
    logs = jnp.where(earlier, between + peaks[:, None, :], -jnp.inf)
    carried_peak = jnp.maximum(since_start, jnp.max(logs, axis=-1))
    mixing = jnp.exp(logs - carried_peak[..., None]).astype(BF16)
    states = everywhere[:, : seqs * cut].reshape(places, seqs, cut * HEAD_DIM)
    carried = dot(mixing, states, (((2,), (0,)), ((0,), (1,)))).astype(BF16)
    carried = carried.transpose(1, 0, 2).reshape(places, seqs * cut, HEAD_DIM)
    carried = exchanged(carried, SP)
    carried = carried.reshape(places, seqs, cut, HEAD_DIM).transpose(1, 0, 2, 3)
    prior_state = carried.reshape(seqs, HEAD_DIM, HEAD_DIM)
    place = lax.axis_index(SP)
    prior_peak = lax.dynamic_slice_in_dim(carried_peak, place, 1, 1)

    conv = project(core_row, pieces, w_conv)
    channels = conv.shape[2] // 3
    gate, mult, inlet = (conv[..., k * channels : (k + 1) * channels] for k in range(3))
    product = (mult.astype(F32) * inlet.astype(F32)).astype(BF16)
    taps = conv_taps.shape[0]
    rim = from_behind(product[:, tokens - (taps - 1) :], SP)
    padded = jnp.concatenate([rim, product], axis=1).astype(F32)
    tap_rows = lax.dynamic_slice_in_dim(conv_taps, head * channels, channels, 1)
    mixed = tap_rows[0] * padded[:, :tokens]
    for j in range(1, taps):
        mixed = mixed + tap_rows[j] * padded[:, j : j + tokens]
    conv_out = (gate.astype(F32) * mixed).astype(BF16)
    last = (((1,), (1,)), ((), ()))
    conv_parts = returned([conv_out[k] for k in range(seqs)], "fs")
    output = sum(dot(a, w[:, :channels], last) for a, w in zip(conv_parts, w_out))

    spans = jnp.arange(tokens)
    causal = spans[:, None] >= spans[None, :]
    pair_logs = jnp.where(
        causal, sums[:, :, None] - sums[:, None, :] + entry[:, None, :], -jnp.inf
    )
    carried_logs = sums + prior_peak
    row_peak = jnp.maximum(carried_logs, jnp.max(pair_logs, axis=-1))
    inner_weights = jnp.exp(pair_logs - row_peak[..., None]) * scale
    carried_weights = jnp.exp(carried_logs - row_peak)
    scores = inner_weights * dot(query, key, (((2,), (2,)), ((0,), (0,))))
    cell = carried_weights[..., None] * dot(query, prior_state, (((2,), (2,)), ((0,), (0,))))
    cell = cell + dot(scores.astype(BF16), value, (((2,), (1,)), ((0,), (0,))))
    cell = cell * lax.rsqrt(jnp.mean(cell * cell, axis=-1, keepdims=True) + EPSILON)
    gain = lax.dynamic_slice_in_dim(head_gain, head * HEAD_DIM, HEAD_DIM, 0)
    mem_out = (cell * gain).astype(BF16)
    mem_parts = returned([mem_out[k] for k in range(seqs)], "fs")
    output = output + sum(dot(a, w[:, channels:], last) for a, w in zip(mem_parts, w_out))

    cores = lax.axis_size("tp")
    parts = exchanged(output.astype(BF16).reshape(cores, tokens // cores, width), "tp")
    return jnp.sum(parts.astype(F32), axis=0).astype(BF16)[None]


def solution(mesh):
    finer = Mesh(
        mesh.devices.reshape(8, 8, mesh.shape["fs"], mesh.shape["tp"]), ("sp_0", "sp_1", "fs", "tp")
    )
    weights = P(SP, ("fs", "tp"))
    return jax.shard_map(
        shards,
        mesh=finer,
        in_specs=(
            P("fs", SP, None),
            P(),
            weights,
            weights,
            weights,
            P(),
            weights,
            weights,
            weights,
            P(),
            P(),
            P(),
            P(None, SP, None),
            P(),
            P(("fs", "tp"), SP),
            P(("fs", "tp"), SP),
        ),
        out_specs=P("fs", SP_TP, None),
        check_vma=False,
    )
```

```python
import jax
import jax.numpy as jnp
from jax import lax
from jax.experimental import pallas as pl
from jax.experimental.pallas import tpu as pltpu
from jax.sharding import Mesh
from jax.sharding import PartitionSpec as P


HEAD_DIM = 128
SP = ("sp_0", "sp_1")
SP_TP = ("sp_0", "sp_1", "tp")
EPSILON = 1e-06
HIGHEST = lax.Precision.HIGHEST
F32 = jnp.float32
BF16 = jnp.bfloat16


def everyone(array, axis):
    copies = jnp.broadcast_to(array, (lax.axis_size(axis), *array.shape))
    return lax.all_to_all(copies, axis, split_axis=0, concat_axis=0, tiled=True)


def exchanged(array, axis):
    return lax.all_to_all(array, axis, split_axis=0, concat_axis=0, tiled=True)


def other_core(array):
    return lax.ppermute(array, "tp", [(0, 1), (1, 0)])


def from_behind(array, axis):
    peers = lax.axis_size(axis)
    return lax.ppermute(array, axis, [(i, i + 1) for i in range(peers - 1)])


def thirds(x):
    first = lax.reduce_precision(x, 8, 7)
    second = lax.reduce_precision(x - first, 8, 7)
    third = lax.reduce_precision(x - first - second, 8, 7)
    return jnp.stack([first, second, third])


def dot(a, b, dims):
    return lax.dot_general(a, b, dims, preferred_element_type=F32)


def ring(array, axis, by):
    peers = lax.axis_size(axis)
    return lax.ppermute(array, axis, [(i, (i + by) % peers) for i in range(peers)])


def around(array, axis):
    behind = ring(array, axis, 1)
    ahead = ring(array, axis, -1)
    cut = array.shape[0] // 2
    far = jnp.concatenate(
        [ring(behind[:cut], axis, 1), ring(ahead[cut:], axis, -1)], axis=0
    )
    return behind, ahead, far


def returned(blocks, axis):
    own, behind, ahead, far = blocks
    return own, ring(ahead, axis, 1), ring(behind, axis, -1), ring(far, axis, 2)


def ring_gather(array, axis):
    behind, ahead = [array], [array]
    for k in range(4):
        behind.append(ring(behind[-1], axis, 1))
        if k < 3:
            ahead.append(ring(ahead[-1], axis, -1))
    return behind + ahead[1:]


OFFSETS = (0, 7, 6, 5, 4, 1, 2, 3)


def matmuls(core, pieces, weights, out):
    half = pieces[0].shape[1]
    first = pl.multiple_of(core * half, half)
    second = pl.multiple_of((1 - core) * half, half)
    for k in range(4):
        mixed = jnp.dot(
            pieces[2 * k][...], weights[pl.ds(first, half), :], preferred_element_type=F32
        )
        mixed += jnp.dot(
            pieces[2 * k + 1][...], weights[pl.ds(second, half), :], preferred_element_type=F32
        )
        out[k] = mixed.astype(BF16)


def project_mem_kernel(spot, *refs):
    parts, pieces, gate_rows = refs[:8], refs[8:16], refs[16]
    out, gates, weights = refs[17:]
    core = spot[0]
    for part, offset in zip(parts, OFFSETS):
        place = (spot[2] + offset) % 8
        for k in range(8):
            start = pl.multiple_of((k * 8 + place) * 32, 32)
            weights[pl.ds(start, 32), :] = part[pl.ds(k * 32, 32), :]
    matmuls(core, pieces, weights, out)
    dims = (((1,), (1,)), ((), ()))
    for k in range(4):
        rows = dot(gate_rows[core], pieces[2 * k][...], dims)
        gates[k] = rows + dot(gate_rows[1 - core], pieces[2 * k + 1][...], dims)


def project_conv_kernel(spot, *refs):
    matmuls(spot[0], refs[:8], refs[8], refs[9])


def arrange_kernel(spot, *refs):
    parts, left, right = refs[:8], refs[8], refs[9]
    wide, size = left.shape[1], parts[0].shape[0]
    for part, offset in zip(parts, OFFSETS):
        start = pl.multiple_of(((spot[1] + offset) % 8) * size, size)
        left[pl.ds(start, size), :] = part[:, :wide]
        right[pl.ds(start, size), :] = part[:, wide:]


def output_kernel(*refs):
    parts, weights, out = refs[:4], refs[4:8], refs[8]
    dims = (((1,), (1,)), ((), ()))
    mixed = dot(parts[0][...], weights[0][...], dims)
    for part, weight in zip(parts[1:], weights[1:]):
        mixed += dot(part[...], weight[...], dims)
    out[...] = mixed.astype(BF16)


def in_vmem(count):
    return [pl.BlockSpec(memory_space=pltpu.VMEM)] * count


def call(kernel, shapes, spot, arrays, flops, scratch=()):
    smem = [pl.BlockSpec(memory_space=pltpu.SMEM)] if spot is not None else []
    return pl.pallas_call(
        kernel,
        out_shape=tuple(jax.ShapeDtypeStruct(shape, dtype) for shape, dtype in shapes),
        in_specs=smem + in_vmem(len(arrays)),
        out_specs=tuple(in_vmem(len(shapes))),
        scratch_shapes=list(scratch),
        cost_estimate=pl.CostEstimate(flops=flops, bytes_accessed=6 << 20, transcendentals=0),
    )(*([spot] if spot is not None else []), *arrays)


def shards(
    activations,
    norm_gain,
    w_conv_gate,
    w_conv_mult,
    w_conv_in,
    conv_taps,
    w_query,
    w_key,
    w_value,
    w_input_gate,
    w_forget_gate,
    gate_bias,
    decay_shift,
    head_gain,
    w_out_conv,
    w_out_mem,
):
    head = lax.axis_index("fs") * lax.axis_size("tp") + lax.axis_index("tp")
    core = lax.axis_index("tp")
    tokens, width = activations.shape[1:]
    half = width // 2
    seqs = lax.axis_size("fs")

    place_x = lax.axis_index("fs")
    order = [(place_x + by) % seqs for by in (0, seqs - 1, 1, 2)]

    spots = [lax.axis_index(name) for name in ("tp", "sp_0", "sp_1")]
    spot = jnp.stack(spots).astype(jnp.int32)

    w_mem = jnp.concatenate([w_query, w_key, w_value], axis=1)
    w_rest = jnp.concatenate(
        [w_conv_gate, w_conv_mult, w_conv_in, w_out_conv.T, w_out_mem.T], axis=1
    )
    channels = w_conv_gate.shape[1]
    w_mem = everyone(w_mem, "sp_0").reshape(-1, w_mem.shape[1])
    w_rest, w_mem = lax.optimization_barrier((w_rest, w_mem))
    w_rest = everyone(w_rest, "sp_1").reshape(-1, w_rest.shape[1])
    w_mem = ring_gather(w_mem, "sp_1")
    w_rest = ring_gather(w_rest, "sp_0")
    w_conv, w_own = call(
        arrange_kernel,
        [((width, 3 * channels), BF16), ((width, 2 * channels), BF16)],
        spot,
        w_rest,
        10**9,
    )
    w_out = (w_own, *around(w_own, "fs"))

    x = activations[0].astype(F32)
    normed = (
        x * lax.rsqrt(jnp.mean(x * x, axis=-1, keepdims=True) + EPSILON) * norm_gain
    ).astype(BF16)
    mine = lax.dynamic_slice_in_dim(normed, core * half, half, 1)
    pieces = [mine, lax.dynamic_slice_in_dim(normed, (1 - core) * half, half, 1)]
    for piece in around(mine, "fs"):
        pieces += [piece, other_core(piece)]

    gate_rows = jnp.concatenate(
        [
            lax.dynamic_slice_in_dim(w_input_gate, head, 1, 1),
            lax.dynamic_slice_in_dim(w_forget_gate, head, 1, 1),
        ],
        axis=1,
    ).T
    gate_rows = jnp.pad(gate_rows, ((0, 14), (0, 0))).reshape(16, 2, half).transpose(1, 0, 2)
    qkv, gates = call(
        project_mem_kernel,
        [((seqs, tokens, 3 * HEAD_DIM), BF16), ((seqs, 16, tokens), F32)],
        spot,
        [*w_mem, *pieces, gate_rows],
        10**9 * 3,
        [pltpu.VMEM((width, 3 * HEAD_DIM), BF16)],
    )
    query, key, value = (qkv[..., k * HEAD_DIM : (k + 1) * HEAD_DIM] for k in range(3))
    bias = lax.dynamic_slice_in_dim(gate_bias, head, 1, 1)
    decay = lax.dynamic_slice_in_dim(decay_shift, head, 1, 2)[..., 0]
    decay = jnp.concatenate([lax.dynamic_slice_in_dim(decay, k, 1, 0) for k in order], axis=0)
    entry = gates[:, 0] + bias[0]
    log_forget = jax.nn.log_sigmoid(gates[:, 1] + bias[1]) + decay
    sums = jnp.cumsum(log_forget, axis=-1)
    total = sums[:, -1]
    local_logs = total[:, None] - sums + entry
    peak = jnp.max(local_logs, axis=-1)
    scale = HEAD_DIM ** (-0.5)
    local_weights = jnp.exp(local_logs - peak[:, None]) * scale

    weighted = (local_weights[..., None] * value.astype(F32)).astype(BF16)
    state = dot(weighted, key, (((1,), (1,)), ((0,), (0,))))

    places = lax.axis_size(SP)
    cut = HEAD_DIM // places
    slices = state.astype(BF16).reshape(seqs, places, cut, HEAD_DIM).transpose(1, 0, 2, 3)
    slices = slices.reshape(places, seqs * cut, HEAD_DIM)
    numbers = thirds(jnp.stack([total, peak])).astype(BF16).reshape(1, 1, -1)
    count = numbers.shape[2]
    numbers = jnp.pad(numbers, ((0, 0), (0, seqs * cut - 1), (0, HEAD_DIM - count)))
    numbers = jnp.broadcast_to(numbers, slices.shape)
    packed = jnp.concatenate([slices, numbers], axis=1)
    everywhere = exchanged(packed, SP)
    found = everywhere[:, seqs * cut, :count].astype(F32).reshape(places, 3, 2, seqs)
    found = found[:, 0] + found[:, 1] + found[:, 2]
    totals, peaks = found[:, 0].T, found[:, 1].T
    line = jnp.arange(places)
    earlier = line[:, None] > line[None, :]
    masked = jnp.where(earlier, totals[:, None, :], 0.0)
    between = lax.dot_general(
        masked, earlier.astype(F32), (((2,), (0,)), ((), ())), precision=HIGHEST
    )
    since_start = jnp.sum(masked, axis=-1)
    logs = jnp.where(earlier, between + peaks[:, None, :], -jnp.inf)
    carried_peak = jnp.maximum(since_start, jnp.max(logs, axis=-1))
    mixing = jnp.exp(logs - carried_peak[..., None]).astype(BF16)
    states = everywhere[:, : seqs * cut].reshape(places, seqs, cut * HEAD_DIM)
    carried = dot(mixing, states, (((2,), (0,)), ((0,), (1,)))).astype(BF16)
    carried = carried.transpose(1, 0, 2).reshape(places, seqs * cut, HEAD_DIM)
    carried = exchanged(carried, SP)
    carried = carried.reshape(places, seqs, cut, HEAD_DIM).transpose(1, 0, 2, 3)
    prior_state = carried.reshape(seqs, HEAD_DIM, HEAD_DIM)
    place = lax.axis_index(SP)
    prior_peak = lax.dynamic_slice_in_dim(carried_peak, place, 1, 1)

    (conv,) = call(
        project_conv_kernel,
        [((seqs, tokens, 3 * channels), BF16)],
        spot,
        [*pieces, w_conv],
        10**9 * 3,
    )
    gate, mult, inlet = (conv[..., k * channels : (k + 1) * channels] for k in range(3))
    product = (mult.astype(F32) * inlet.astype(F32)).astype(BF16)
    taps = conv_taps.shape[0]
    rim = from_behind(product[:, tokens - (taps - 1) :], SP)
    padded = jnp.concatenate([rim, product], axis=1).astype(F32)
    tap_rows = lax.dynamic_slice_in_dim(conv_taps, head * channels, channels, 1)
    mixed = tap_rows[0] * padded[:, :tokens]
    for j in range(1, taps):
        mixed = mixed + tap_rows[j] * padded[:, j : j + tokens]
    conv_out = (gate.astype(F32) * mixed).astype(BF16)
    spans = jnp.arange(tokens)
    causal = spans[:, None] >= spans[None, :]
    pair_logs = jnp.where(
        causal, sums[:, :, None] - sums[:, None, :] + entry[:, None, :], -jnp.inf
    )
    carried_logs = sums + prior_peak
    row_peak = jnp.maximum(carried_logs, jnp.max(pair_logs, axis=-1))
    inner_weights = jnp.exp(pair_logs - row_peak[..., None]) * scale
    carried_weights = jnp.exp(carried_logs - row_peak)
    scores = inner_weights * dot(query, key, (((2,), (2,)), ((0,), (0,))))
    cell = carried_weights[..., None] * dot(query, prior_state, (((2,), (2,)), ((0,), (0,))))
    cell = cell + dot(scores.astype(BF16), value, (((2,), (1,)), ((0,), (0,))))
    cell = cell * lax.rsqrt(jnp.mean(cell * cell, axis=-1, keepdims=True) + EPSILON)
    gain = lax.dynamic_slice_in_dim(head_gain, head * HEAD_DIM, HEAD_DIM, 0)
    mem_out = (cell * gain).astype(BF16)
    both = jnp.concatenate([conv_out, mem_out], axis=-1)
    parts = returned([both[k] for k in range(seqs)], "fs")
    (output,) = call(output_kernel, [((tokens, width), BF16)], None, [*parts, *w_out], 10**9 * 2)

    cores = lax.axis_size("tp")
    parts = exchanged(output.reshape(cores, tokens // cores, width), "tp")
    return jnp.sum(parts.astype(F32), axis=0).astype(BF16)[None]


def solution(mesh):
    finer = Mesh(
        mesh.devices.reshape(8, 8, mesh.shape["fs"], mesh.shape["tp"]), ("sp_0", "sp_1", "fs", "tp")
    )
    weights = P(SP, ("fs", "tp"))
    return jax.shard_map(
        shards,
        mesh=finer,
        in_specs=(
            P("fs", SP, None),
            P(),
            weights,
            weights,
            weights,
            P(),
            weights,
            weights,
            weights,
            P(),
            P(),
            P(),
            P(None, SP, None),
            P(),
            P(("fs", "tp"), SP),
            P(("fs", "tp"), SP),
        ),
        out_specs=P("fs", SP_TP, None),
        check_vma=False,
    )
```

```python
import jax
import jax.numpy as jnp
from jax import lax
from jax.experimental import pallas as pl
from jax.experimental.pallas import tpu as pltpu
from jax.sharding import Mesh
from jax.sharding import PartitionSpec as P


HEAD_DIM = 128
SP = ("sp_0", "sp_1")
SP_TP = ("sp_0", "sp_1", "tp")
EPSILON = 1e-06
HIGHEST = lax.Precision.HIGHEST
F32 = jnp.float32
BF16 = jnp.bfloat16


def everyone(array, axis):
    copies = jnp.broadcast_to(array, (lax.axis_size(axis), *array.shape))
    return lax.all_to_all(copies, axis, split_axis=0, concat_axis=0, tiled=True)


def exchanged(array, axis):
    return lax.all_to_all(array, axis, split_axis=0, concat_axis=0, tiled=True)


def other_core(array):
    return lax.ppermute(array, "tp", [(0, 1), (1, 0)])


def from_behind(array, axis):
    peers = lax.axis_size(axis)
    return lax.ppermute(array, axis, [(i, i + 1) for i in range(peers - 1)])


def thirds(x):
    first = lax.reduce_precision(x, 8, 7)
    second = lax.reduce_precision(x - first, 8, 7)
    third = lax.reduce_precision(x - first - second, 8, 7)
    return jnp.stack([first, second, third])


def dot(a, b, dims):
    return lax.dot_general(a, b, dims, preferred_element_type=F32)


def ring(array, axis, by):
    peers = lax.axis_size(axis)
    return lax.ppermute(array, axis, [(i, (i + by) % peers) for i in range(peers)])


def around(array, axis):
    return ring(array, axis, -1), ring(array, axis, 2), ring(array, axis, 1)


def rolled(array, by):
    size = array.shape[0]
    twice = jnp.concatenate([array, array], axis=0)
    return lax.dynamic_slice_in_dim(twice, (size - by) % size, size, 0)


def matmuls(core, pieces, weights, left, out):
    half = pieces[0].shape[1]
    first = pl.multiple_of(core * half, half)
    second = pl.multiple_of((1 - core) * half, half)
    right = left + out.shape[2]
    for k in range(4):
        mixed = jnp.dot(
            pieces[2 * k][...],
            weights[pl.ds(first, half), left:right],
            preferred_element_type=F32,
        )
        mixed += jnp.dot(
            pieces[2 * k + 1][...],
            weights[pl.ds(second, half), left:right],
            preferred_element_type=F32,
        )
        out[k] = mixed.astype(BF16)


def project_mem_kernel(spot, *refs):
    pieces, weights, gate_rows, out, gates = refs[:8], refs[8], refs[9], refs[10], refs[11]
    core = spot[0]
    matmuls(core, pieces, weights, 0, out)
    dims = (((1,), (1,)), ((), ()))
    for k in range(4):
        rows = dot(gate_rows[core], pieces[2 * k][...], dims)
        gates[k] = rows + dot(gate_rows[1 - core], pieces[2 * k + 1][...], dims)


def project_conv_kernel(spot, *refs):
    matmuls(spot[0], refs[:8], refs[8], refs[9].shape[2], refs[9])


def output_kernel(parts, weights, out):
    dims = (((1,), (1,)), ((), ()))
    wide = parts.shape[2]
    mixed = dot(parts[0], weights[:, :wide], dims)
    for k in range(1, parts.shape[0]):
        mixed += dot(parts[k], weights[:, k * wide : (k + 1) * wide], dims)
    out[...] = mixed.astype(BF16)


def in_vmem(count):
    return [pl.BlockSpec(memory_space=pltpu.VMEM)] * count


def call(kernel, shapes, spot, arrays, flops, scratch=()):
    smem = [pl.BlockSpec(memory_space=pltpu.SMEM)] if spot is not None else []
    return pl.pallas_call(
        kernel,
        out_shape=tuple(jax.ShapeDtypeStruct(shape, dtype) for shape, dtype in shapes),
        in_specs=smem + in_vmem(len(arrays)),
        out_specs=tuple(in_vmem(len(shapes))),
        scratch_shapes=list(scratch),
        cost_estimate=pl.CostEstimate(flops=flops, bytes_accessed=6 << 20, transcendentals=0),
    )(*([spot] if spot is not None else []), *arrays)


def shards(
    activations,
    norm_gain,
    w_conv_gate,
    w_conv_mult,
    w_conv_in,
    conv_taps,
    w_query,
    w_key,
    w_value,
    w_input_gate,
    w_forget_gate,
    gate_bias,
    decay_shift,
    head_gain,
    w_out_conv,
    w_out_mem,
):
    head = lax.axis_index("fs") * lax.axis_size("tp") + lax.axis_index("tp")
    core = lax.axis_index("tp")
    tokens, width = activations.shape[1:]
    half = width // 2
    seqs = lax.axis_size("fs")

    place_x = lax.axis_index("fs")
    order = [(place_x + by) % seqs for by in range(seqs)]

    spot = core.reshape(1).astype(jnp.int32)

    w_all = jnp.concatenate(
        [w_query, w_key, w_value, w_conv_gate, w_conv_mult, w_conv_in], axis=1
    )
    channels = w_conv_gate.shape[1]
    w_all = everyone(w_all, SP).reshape(width, -1)

    x = activations[0].astype(F32)
    normed = (
        x * lax.rsqrt(jnp.mean(x * x, axis=-1, keepdims=True) + EPSILON) * norm_gain
    ).astype(BF16)
    mine = lax.dynamic_slice_in_dim(normed, core * half, half, 1)
    pieces = [mine, lax.dynamic_slice_in_dim(normed, (1 - core) * half, half, 1)]
    others = around(mine, "fs")
    swapped = other_core(jnp.concatenate(others, axis=0))
    for k, piece in enumerate(others):
        pieces += [piece, swapped[k * tokens : (k + 1) * tokens]]

    turned = jnp.concatenate([w_out_conv.T, w_out_mem.T], axis=1)
    turned = jnp.stack([turned, *around(turned, "fs")])
    turned = rolled(turned, place_x).transpose(1, 0, 2).reshape(turned.shape[1], -1)
    w_out = lax.all_gather(turned, SP, axis=0, tiled=True)

    gate_rows = jnp.concatenate(
        [
            lax.dynamic_slice_in_dim(w_input_gate, head, 1, 1),
            lax.dynamic_slice_in_dim(w_forget_gate, head, 1, 1),
        ],
        axis=1,
    ).T
    gate_rows = jnp.pad(gate_rows, ((0, 14), (0, 0))).reshape(16, 2, half).transpose(1, 0, 2)
    qkv, gates = call(
        project_mem_kernel,
        [((seqs, tokens, 3 * HEAD_DIM), BF16), ((seqs, 16, tokens), F32)],
        spot,
        [*pieces, w_all, gate_rows],
        10**9 * 3,
    )
    query, key, value = (qkv[..., k * HEAD_DIM : (k + 1) * HEAD_DIM] for k in range(3))
    bias = lax.dynamic_slice_in_dim(gate_bias, head, 1, 1)
    decay = lax.dynamic_slice_in_dim(decay_shift, head, 1, 2)[..., 0]
    decay = jnp.concatenate([lax.dynamic_slice_in_dim(decay, k, 1, 0) for k in order], axis=0)
    entry = gates[:, 0] + bias[0]
    log_forget = jax.nn.log_sigmoid(gates[:, 1] + bias[1]) + decay
    sums = jnp.cumsum(log_forget, axis=-1)
    total = sums[:, -1]
    local_logs = total[:, None] - sums + entry
    peak = jnp.max(local_logs, axis=-1)
    scale = HEAD_DIM ** (-0.5)
    local_weights = jnp.exp(local_logs - peak[:, None]) * scale

    weighted = (local_weights[..., None] * value.astype(F32)).astype(BF16)
    state = dot(weighted, key, (((1,), (1,)), ((0,), (0,))))

    places = lax.axis_size(SP)
    cut = HEAD_DIM // places
    slices = state.astype(BF16).reshape(seqs, places, cut, HEAD_DIM).transpose(1, 0, 2, 3)
    slices = slices.reshape(places, seqs * cut, HEAD_DIM)
    numbers = thirds(jnp.stack([total, peak])).astype(BF16).reshape(1, 1, -1)
    count = numbers.shape[2]
    numbers = jnp.pad(numbers, ((0, 0), (0, seqs * cut - 1), (0, HEAD_DIM - count)))
    numbers = jnp.broadcast_to(numbers, slices.shape)
    packed = jnp.concatenate([slices, numbers], axis=1)
    everywhere = exchanged(packed, SP)
    found = everywhere[:, seqs * cut, :count].astype(F32).reshape(places, 3, 2, seqs)
    found = found[:, 0] + found[:, 1] + found[:, 2]
    totals, peaks = found[:, 0].T, found[:, 1].T
    line = jnp.arange(places)
    earlier = line[:, None] > line[None, :]
    masked = jnp.where(earlier, totals[:, None, :], 0.0)
    between = lax.dot_general(
        masked, earlier.astype(F32), (((2,), (0,)), ((), ())), precision=HIGHEST
    )
    since_start = jnp.sum(masked, axis=-1)
    logs = jnp.where(earlier, between + peaks[:, None, :], -jnp.inf)
    carried_peak = jnp.maximum(since_start, jnp.max(logs, axis=-1))
    mixing = jnp.exp(logs - carried_peak[..., None]).astype(BF16)
    states = everywhere[:, : seqs * cut].reshape(places, seqs, cut * HEAD_DIM)
    carried = dot(mixing, states, (((2,), (0,)), ((0,), (1,)))).astype(BF16)
    carried = carried.transpose(1, 0, 2).reshape(places, seqs * cut, HEAD_DIM)
    carried = exchanged(carried, SP)
    carried = carried.reshape(places, seqs, cut, HEAD_DIM).transpose(1, 0, 2, 3)
    prior_state = carried.reshape(seqs, HEAD_DIM, HEAD_DIM)
    place = lax.axis_index(SP)
    prior_peak = lax.dynamic_slice_in_dim(carried_peak, place, 1, 1)

    (conv,) = call(
        project_conv_kernel,
        [((seqs, tokens, 3 * channels), BF16)],
        spot,
        [*pieces, w_all],
        10**9 * 3,
    )
    gate, mult, inlet = (conv[..., k * channels : (k + 1) * channels] for k in range(3))
    product = (mult.astype(F32) * inlet.astype(F32)).astype(BF16)
    taps = conv_taps.shape[0]
    rim = from_behind(product[:, tokens - (taps - 1) :], SP)
    padded = jnp.concatenate([rim, product], axis=1).astype(F32)
    tap_rows = lax.dynamic_slice_in_dim(conv_taps, head * channels, channels, 1)
    mixed = tap_rows[0] * padded[:, :tokens]
    for j in range(1, taps):
        mixed = mixed + tap_rows[j] * padded[:, j : j + tokens]
    conv_out = (gate.astype(F32) * mixed).astype(BF16)
    spans = jnp.arange(tokens)
    causal = spans[:, None] >= spans[None, :]
    pair_logs = jnp.where(
        causal, sums[:, :, None] - sums[:, None, :] + entry[:, None, :], -jnp.inf
    )
    carried_logs = sums + prior_peak
    row_peak = jnp.maximum(carried_logs, jnp.max(pair_logs, axis=-1))
    inner_weights = jnp.exp(pair_logs - row_peak[..., None]) * scale
    carried_weights = jnp.exp(carried_logs - row_peak)
    scores = inner_weights * dot(query, key, (((2,), (2,)), ((0,), (0,))))
    cell = carried_weights[..., None] * dot(query, prior_state, (((2,), (2,)), ((0,), (0,))))
    cell = cell + dot(scores.astype(BF16), value, (((2,), (1,)), ((0,), (0,))))
    cell = cell * lax.rsqrt(jnp.mean(cell * cell, axis=-1, keepdims=True) + EPSILON)
    gain = lax.dynamic_slice_in_dim(head_gain, head * HEAD_DIM, HEAD_DIM, 0)
    mem_out = (cell * gain).astype(BF16)
    both = rolled(jnp.concatenate([conv_out, mem_out], axis=-1), place_x)
    both = exchanged(both, "fs")
    (output,) = call(
        output_kernel, [((tokens, width), BF16)], None, [both, w_out], 10**9 * 2
    )

    cores = lax.axis_size("tp")
    parts = exchanged(output.reshape(cores, tokens // cores, width), "tp")
    return jnp.sum(parts.astype(F32), axis=0).astype(BF16)[None]


def solution(mesh):
    finer = Mesh(
        mesh.devices.reshape(8, 8, mesh.shape["fs"], mesh.shape["tp"]), ("sp_0", "sp_1", "fs", "tp")
    )
    weights = P(SP, ("fs", "tp"))
    return jax.shard_map(
        shards,
        mesh=finer,
        in_specs=(
            P("fs", SP, None),
            P(),
            weights,
            weights,
            weights,
            P(),
            weights,
            weights,
            weights,
            P(),
            P(),
            P(),
            P(None, SP, None),
            P(),
            P(("fs", "tp"), SP),
            P(("fs", "tp"), SP),
        ),
        out_specs=P("fs", SP_TP, None),
        check_vma=False,
    )
```

```python
import jax
import jax.numpy as jnp
from jax import lax
from jax.experimental import pallas as pl
from jax.experimental.pallas import tpu as pltpu
from jax.sharding import Mesh
from jax.sharding import PartitionSpec as P


HEAD_DIM = 128
SP = ("sp_0", "sp_1")
SP_TP = ("sp_0", "sp_1", "tp")
EPSILON = 1e-06
HIGHEST = lax.Precision.HIGHEST
F32 = jnp.float32
BF16 = jnp.bfloat16


def everyone(array, axis):
    copies = jnp.broadcast_to(array, (lax.axis_size(axis), *array.shape))
    return lax.all_to_all(copies, axis, split_axis=0, concat_axis=0, tiled=True)


def exchanged(array, axis):
    return lax.all_to_all(array, axis, split_axis=0, concat_axis=0, tiled=True)


def other_core(array):
    return lax.ppermute(array, "tp", [(0, 1), (1, 0)])


def from_behind(array, axis):
    peers = lax.axis_size(axis)
    return lax.ppermute(array, axis, [(i, i + 1) for i in range(peers - 1)])


def thirds(x):
    first = lax.reduce_precision(x, 8, 7)
    second = lax.reduce_precision(x - first, 8, 7)
    third = lax.reduce_precision(x - first - second, 8, 7)
    return jnp.stack([first, second, third])


def dot(a, b, dims):
    return lax.dot_general(a, b, dims, preferred_element_type=F32)


def ring(array, axis, by):
    peers = lax.axis_size(axis)
    return lax.ppermute(array, axis, [(i, (i + by) % peers) for i in range(peers)])


def around(array, axis):
    return ring(array, axis, -1), ring(array, axis, 2), ring(array, axis, 1)


def relayed(array, axis):
    cut = array.shape[0] // 2
    ahead = ring(array, axis, -1)
    behind = ring(array, axis, 1)
    first = ring(behind[:cut], axis, 1)
    second = ring(ahead[cut:], axis, -1)
    return ahead, jnp.concatenate([first, second], axis=0), behind


def rolled(array, by):
    size = array.shape[0]
    twice = jnp.concatenate([array, array], axis=0)
    return lax.dynamic_slice_in_dim(twice, (size - by) % size, size, 0)


def matmuls(core, pieces, weights, left, out):
    half = pieces[0].shape[1]
    first = pl.multiple_of(core * half, half)
    second = pl.multiple_of((1 - core) * half, half)
    right = left + out.shape[2]
    for k in range(4):
        mixed = jnp.dot(
            pieces[2 * k][...],
            weights[pl.ds(first, half), left:right],
            preferred_element_type=F32,
        )
        mixed += jnp.dot(
            pieces[2 * k + 1][...],
            weights[pl.ds(second, half), left:right],
            preferred_element_type=F32,
        )
        out[k] = mixed.astype(BF16)


def project_mem_kernel(spot, *refs):
    pieces, weights, gate_rows, out, gates = refs[:8], refs[8], refs[9], refs[10], refs[11]
    core = spot[0]
    matmuls(core, pieces, weights, 0, out)
    dims = (((1,), (1,)), ((), ()))
    for k in range(4):
        rows = dot(gate_rows[core], pieces[2 * k][...], dims)
        gates[k] = rows + dot(gate_rows[1 - core], pieces[2 * k + 1][...], dims)


def project_conv_kernel(spot, *refs):
    matmuls(spot[0], refs[:8], refs[8], refs[9].shape[2], refs[9])


def output_kernel(spot, parts, *refs):
    weights, out = refs[:4], refs[4]
    dims = (((1,), (1,)), ((), ()))
    mixed = dot(parts[spot[1]], weights[0][...], dims)
    for k in range(1, 4):
        mixed += dot(parts[(spot[1] + k) % 4], weights[k][...], dims)
    out[...] = mixed.astype(BF16)


def in_vmem(count):
    return [pl.BlockSpec(memory_space=pltpu.VMEM)] * count


def call(kernel, shapes, spot, arrays, flops, scratch=()):
    smem = [pl.BlockSpec(memory_space=pltpu.SMEM)] if spot is not None else []
    return pl.pallas_call(
        kernel,
        out_shape=tuple(jax.ShapeDtypeStruct(shape, dtype) for shape, dtype in shapes),
        in_specs=smem + in_vmem(len(arrays)),
        out_specs=tuple(in_vmem(len(shapes))),
        scratch_shapes=list(scratch),
        cost_estimate=pl.CostEstimate(flops=flops, bytes_accessed=6 << 20, transcendentals=0),
    )(*([spot] if spot is not None else []), *arrays)


def shards(
    activations,
    norm_gain,
    w_conv_gate,
    w_conv_mult,
    w_conv_in,
    conv_taps,
    w_query,
    w_key,
    w_value,
    w_input_gate,
    w_forget_gate,
    gate_bias,
    decay_shift,
    head_gain,
    w_out_conv,
    w_out_mem,
):
    head = lax.axis_index("fs") * lax.axis_size("tp") + lax.axis_index("tp")
    core = lax.axis_index("tp")
    tokens, width = activations.shape[1:]
    half = width // 2
    seqs = lax.axis_size("fs")

    place_x = lax.axis_index("fs")
    order = [(place_x + by) % seqs for by in range(seqs)]

    spot = jnp.stack([core, place_x]).astype(jnp.int32)

    w_all = jnp.concatenate(
        [
            w_query,
            w_key,
            w_value,
            w_conv_gate,
            w_conv_mult,
            w_conv_in,
            w_out_conv.T,
            w_out_mem.T,
        ],
        axis=1,
    )
    channels = w_conv_gate.shape[1]
    w_all = everyone(w_all, SP).reshape(width, -1)
    w_own = w_all[:, 6 * channels :]
    w_out = (w_own, *relayed(w_own, "fs"))

    x = activations[0].astype(F32)
    normed = (
        x * lax.rsqrt(jnp.mean(x * x, axis=-1, keepdims=True) + EPSILON) * norm_gain
    ).astype(BF16)
    mine = lax.dynamic_slice_in_dim(normed, core * half, half, 1)
    pieces = [mine, lax.dynamic_slice_in_dim(normed, (1 - core) * half, half, 1)]
    others = around(mine, "fs")
    swapped = other_core(jnp.concatenate(others, axis=0))
    for k, piece in enumerate(others):
        pieces += [piece, swapped[k * tokens : (k + 1) * tokens]]

    gate_rows = jnp.concatenate(
        [
            lax.dynamic_slice_in_dim(w_input_gate, head, 1, 1),
            lax.dynamic_slice_in_dim(w_forget_gate, head, 1, 1),
        ],
        axis=1,
    ).T
    gate_rows = jnp.pad(gate_rows, ((0, 14), (0, 0))).reshape(16, 2, half).transpose(1, 0, 2)
    qkv, gates = call(
        project_mem_kernel,
        [((seqs, tokens, 3 * HEAD_DIM), BF16), ((seqs, 16, tokens), F32)],
        spot,
        [*pieces, w_all, gate_rows],
        10**9 * 3,
    )
    query, key, value = (qkv[..., k * HEAD_DIM : (k + 1) * HEAD_DIM] for k in range(3))
    bias = lax.dynamic_slice_in_dim(gate_bias, head, 1, 1)
    decay = lax.dynamic_slice_in_dim(decay_shift, head, 1, 2)[..., 0]
    decay = jnp.concatenate([lax.dynamic_slice_in_dim(decay, k, 1, 0) for k in order], axis=0)
    entry = gates[:, 0] + bias[0]
    log_forget = jax.nn.log_sigmoid(gates[:, 1] + bias[1]) + decay
    sums = jnp.cumsum(log_forget, axis=-1)
    total = sums[:, -1]
    local_logs = total[:, None] - sums + entry
    peak = jnp.max(local_logs, axis=-1)
    scale = HEAD_DIM ** (-0.5)
    local_weights = jnp.exp(local_logs - peak[:, None]) * scale

    weighted = (local_weights[..., None] * value.astype(F32)).astype(BF16)
    state = dot(weighted, key, (((1,), (1,)), ((0,), (0,))))

    places = lax.axis_size(SP)
    cut = HEAD_DIM // places
    slices = state.astype(BF16).reshape(seqs, places, cut, HEAD_DIM).transpose(1, 0, 2, 3)
    slices = slices.reshape(places, seqs * cut, HEAD_DIM)
    numbers = thirds(jnp.stack([total, peak])).astype(BF16).reshape(1, 1, -1)
    count = numbers.shape[2]
    numbers = jnp.pad(numbers, ((0, 0), (0, seqs * cut - 1), (0, HEAD_DIM - count)))
    numbers = jnp.broadcast_to(numbers, slices.shape)
    packed = jnp.concatenate([slices, numbers], axis=1)
    everywhere = exchanged(packed, SP)
    found = everywhere[:, seqs * cut, :count].astype(F32).reshape(places, 3, 2, seqs)
    found = found[:, 0] + found[:, 1] + found[:, 2]
    totals, peaks = found[:, 0].T, found[:, 1].T
    line = jnp.arange(places)
    earlier = line[:, None] > line[None, :]
    masked = jnp.where(earlier, totals[:, None, :], 0.0)
    between = lax.dot_general(
        masked, earlier.astype(F32), (((2,), (0,)), ((), ())), precision=HIGHEST
    )
    since_start = jnp.sum(masked, axis=-1)
    logs = jnp.where(earlier, between + peaks[:, None, :], -jnp.inf)
    carried_peak = jnp.maximum(since_start, jnp.max(logs, axis=-1))
    mixing = jnp.exp(logs - carried_peak[..., None]).astype(BF16)
    states = everywhere[:, : seqs * cut].reshape(places, seqs, cut * HEAD_DIM)
    carried = dot(mixing, states, (((2,), (0,)), ((0,), (1,)))).astype(BF16)
    carried = carried.transpose(1, 0, 2).reshape(places, seqs * cut, HEAD_DIM)
    carried = exchanged(carried, SP)
    carried = carried.reshape(places, seqs, cut, HEAD_DIM).transpose(1, 0, 2, 3)
    prior_state = carried.reshape(seqs, HEAD_DIM, HEAD_DIM)
    place = lax.axis_index(SP)
    prior_peak = lax.dynamic_slice_in_dim(carried_peak, place, 1, 1)

    (conv,) = call(
        project_conv_kernel,
        [((seqs, tokens, 3 * channels), BF16)],
        spot,
        [*pieces, w_all],
        10**9 * 3,
    )
    gate, mult, inlet = (conv[..., k * channels : (k + 1) * channels] for k in range(3))
    product = (mult.astype(F32) * inlet.astype(F32)).astype(BF16)
    taps = conv_taps.shape[0]
    rim = from_behind(product[:, tokens - (taps - 1) :], SP)
    padded = jnp.concatenate([rim, product], axis=1).astype(F32)
    tap_rows = lax.dynamic_slice_in_dim(conv_taps, head * channels, channels, 1)
    mixed = tap_rows[0] * padded[:, :tokens]
    for j in range(1, taps):
        mixed = mixed + tap_rows[j] * padded[:, j : j + tokens]
    conv_out = (gate.astype(F32) * mixed).astype(BF16)
    spans = jnp.arange(tokens)
    causal = spans[:, None] >= spans[None, :]
    pair_logs = jnp.where(
        causal, sums[:, :, None] - sums[:, None, :] + entry[:, None, :], -jnp.inf
    )
    carried_logs = sums + prior_peak
    row_peak = jnp.maximum(carried_logs, jnp.max(pair_logs, axis=-1))
    inner_weights = jnp.exp(pair_logs - row_peak[..., None]) * scale
    carried_weights = jnp.exp(carried_logs - row_peak)
    scores = inner_weights * dot(query, key, (((2,), (2,)), ((0,), (0,))))
    cell = carried_weights[..., None] * dot(query, prior_state, (((2,), (2,)), ((0,), (0,))))
    cell = cell + dot(scores.astype(BF16), value, (((2,), (1,)), ((0,), (0,))))
    cell = cell * lax.rsqrt(jnp.mean(cell * cell, axis=-1, keepdims=True) + EPSILON)
    gain = lax.dynamic_slice_in_dim(head_gain, head * HEAD_DIM, HEAD_DIM, 0)
    mem_out = (cell * gain).astype(BF16)
    both = rolled(jnp.concatenate([conv_out, mem_out], axis=-1), place_x)
    both = exchanged(both, "fs")
    (output,) = call(
        output_kernel, [((tokens, width), BF16)], spot, [both, *w_out], 10**9 * 2
    )

    cores = lax.axis_size("tp")
    parts = exchanged(output.reshape(cores, tokens // cores, width), "tp")
    return jnp.sum(parts.astype(F32), axis=0).astype(BF16)[None]


def solution(mesh):
    finer = Mesh(
        mesh.devices.reshape(8, 8, mesh.shape["fs"], mesh.shape["tp"]), ("sp_0", "sp_1", "fs", "tp")
    )
    weights = P(SP, ("fs", "tp"))
    return jax.shard_map(
        shards,
        mesh=finer,
        in_specs=(
            P("fs", SP, None),
            P(),
            weights,
            weights,
            weights,
            P(),
            weights,
            weights,
            weights,
            P(),
            P(),
            P(),
            P(None, SP, None),
            P(),
            P(("fs", "tp"), SP),
            P(("fs", "tp"), SP),
        ),
        out_specs=P("fs", SP_TP, None),
        check_vma=False,
    )
```

```python
import jax
import jax.numpy as jnp
from jax import lax
from jax.experimental import pallas as pl
from jax.experimental.pallas import tpu as pltpu
from jax.sharding import Mesh
from jax.sharding import PartitionSpec as P


HEAD_DIM = 128
SP = ("sp_0", "sp_1")
SP_TP = ("sp_0", "sp_1", "tp")
EPSILON = 1e-06
HIGHEST = lax.Precision.HIGHEST
F32 = jnp.float32
BF16 = jnp.bfloat16


def everyone(array, axis):
    copies = jnp.broadcast_to(array, (lax.axis_size(axis), *array.shape))
    return lax.all_to_all(copies, axis, split_axis=0, concat_axis=0, tiled=True)


def exchanged(array, axis):
    return lax.all_to_all(array, axis, split_axis=0, concat_axis=0, tiled=True)


def other_core(array):
    return lax.ppermute(array, "tp", [(0, 1), (1, 0)])


def from_behind(array, axis):
    peers = lax.axis_size(axis)
    return lax.ppermute(array, axis, [(i, i + 1) for i in range(peers - 1)])


def thirds(x):
    first = lax.reduce_precision(x, 8, 7)
    second = lax.reduce_precision(x - first, 8, 7)
    third = lax.reduce_precision(x - first - second, 8, 7)
    return jnp.stack([first, second, third])


def dot(a, b, dims):
    return lax.dot_general(a, b, dims, preferred_element_type=F32)


def ring(array, axis, by):
    peers = lax.axis_size(axis)
    return lax.ppermute(array, axis, [(i, (i + by) % peers) for i in range(peers)])


def around(array, axis):
    return ring(array, axis, -1), ring(array, axis, 2), ring(array, axis, 1)


def relayed(array, axis):
    cut = array.shape[0] // 2
    ahead = ring(array, axis, -1)
    behind = ring(array, axis, 1)
    first = ring(behind[:cut], axis, 1)
    second = ring(ahead[cut:], axis, -1)
    return ahead, jnp.concatenate([first, second], axis=0), behind


def rolled(array, by):
    size = array.shape[0]
    twice = jnp.concatenate([array, array], axis=0)
    return lax.dynamic_slice_in_dim(twice, (size - by) % size, size, 0)


def ring_gather(array, axis):
    behind, ahead = [array], [array]
    for k in range(4):
        behind.append(ring(behind[-1], axis, 1))
        if k < 3:
            ahead.append(ring(ahead[-1], axis, -1))
    return behind + ahead[1:]


OFFSETS = (0, 7, 6, 5, 4, 1, 2, 3)


def matmuls(core, pieces, weights, left, out):
    half = pieces[0].shape[1]
    first = pl.multiple_of(core * half, half)
    second = pl.multiple_of((1 - core) * half, half)
    right = left + out.shape[2]
    for k in range(4):
        mixed = jnp.dot(
            pieces[2 * k][...],
            weights[pl.ds(first, half), left:right],
            preferred_element_type=F32,
        )
        mixed += jnp.dot(
            pieces[2 * k + 1][...],
            weights[pl.ds(second, half), left:right],
            preferred_element_type=F32,
        )
        out[k] = mixed.astype(BF16)


def project_mem_kernel(spot, *refs):
    parts, pieces, gate_rows = refs[:8], refs[8:16], refs[16]
    out, gates, weights = refs[17:]
    core = spot[0]
    for part, offset in zip(parts, OFFSETS):
        place = (spot[2] + offset) % 8
        for k in range(8):
            start = pl.multiple_of((k * 8 + place) * 32, 32)
            weights[pl.ds(start, 32), :] = part[pl.ds(k * 32, 32), :]
    matmuls(core, pieces, weights, 0, out)
    dims = (((1,), (1,)), ((), ()))
    for k in range(4):
        rows = dot(gate_rows[core], pieces[2 * k][...], dims)
        gates[k] = rows + dot(gate_rows[1 - core], pieces[2 * k + 1][...], dims)


def project_conv_kernel(spot, *refs):
    matmuls(spot[0], refs[:8], refs[8], 0, refs[9])


def output_kernel(spot, parts, *refs):
    weights, out = refs[:4], refs[4]
    dims = (((1,), (1,)), ((), ()))
    mixed = dot(parts[spot[1]], weights[0][...], dims)
    for k in range(1, 4):
        mixed += dot(parts[(spot[1] + k) % 4], weights[k][...], dims)
    out[...] = mixed.astype(BF16)


def in_vmem(count):
    return [pl.BlockSpec(memory_space=pltpu.VMEM)] * count


def call(kernel, shapes, spot, arrays, flops, scratch=()):
    smem = [pl.BlockSpec(memory_space=pltpu.SMEM)] if spot is not None else []
    return pl.pallas_call(
        kernel,
        out_shape=tuple(jax.ShapeDtypeStruct(shape, dtype) for shape, dtype in shapes),
        in_specs=smem + in_vmem(len(arrays)),
        out_specs=tuple(in_vmem(len(shapes))),
        scratch_shapes=list(scratch),
        cost_estimate=pl.CostEstimate(flops=flops, bytes_accessed=6 << 20, transcendentals=0),
    )(*([spot] if spot is not None else []), *arrays)


def shards(
    activations,
    norm_gain,
    w_conv_gate,
    w_conv_mult,
    w_conv_in,
    conv_taps,
    w_query,
    w_key,
    w_value,
    w_input_gate,
    w_forget_gate,
    gate_bias,
    decay_shift,
    head_gain,
    w_out_conv,
    w_out_mem,
):
    head = lax.axis_index("fs") * lax.axis_size("tp") + lax.axis_index("tp")
    core = lax.axis_index("tp")
    tokens, width = activations.shape[1:]
    half = width // 2
    seqs = lax.axis_size("fs")

    place_x = lax.axis_index("fs")
    order = [(place_x + by) % seqs for by in range(seqs)]

    place_y = lax.axis_index("sp_1")
    spot = jnp.stack([core, place_x, place_y]).astype(jnp.int32)

    channels = w_conv_gate.shape[1]
    w_rest = jnp.concatenate(
        [w_conv_gate, w_conv_mult, w_conv_in, w_out_conv.T, w_out_mem.T], axis=1
    )
    w_mem = jnp.concatenate([w_query, w_key, w_value], axis=1)
    w_rest, w_mem = lax.optimization_barrier((w_rest, w_mem))
    w_mem = everyone(w_mem, "sp_0").reshape(-1, w_mem.shape[1])
    w_mem = ring_gather(w_mem, "sp_1")

    w_rest = lax.all_gather(w_rest, SP, axis=0, tiled=True)
    w_own = w_rest[:, 3 * channels :]
    w_out = (w_own, *relayed(w_own, "fs"))

    x = activations[0].astype(F32)
    normed = (
        x * lax.rsqrt(jnp.mean(x * x, axis=-1, keepdims=True) + EPSILON) * norm_gain
    ).astype(BF16)
    mine = lax.dynamic_slice_in_dim(normed, core * half, half, 1)
    pieces = [mine, lax.dynamic_slice_in_dim(normed, (1 - core) * half, half, 1)]
    others = around(mine, "fs")
    swapped = other_core(jnp.concatenate(others, axis=0))
    for k, piece in enumerate(others):
        pieces += [piece, swapped[k * tokens : (k + 1) * tokens]]

    gate_rows = jnp.concatenate(
        [
            lax.dynamic_slice_in_dim(w_input_gate, head, 1, 1),
            lax.dynamic_slice_in_dim(w_forget_gate, head, 1, 1),
        ],
        axis=1,
    ).T
    gate_rows = jnp.pad(gate_rows, ((0, 14), (0, 0))).reshape(16, 2, half).transpose(1, 0, 2)
    qkv, gates = call(
        project_mem_kernel,
        [((seqs, tokens, 3 * HEAD_DIM), BF16), ((seqs, 16, tokens), F32)],
        spot,
        [*w_mem, *pieces, gate_rows],
        10**9 * 3,
        [pltpu.VMEM((width, 3 * HEAD_DIM), BF16)],
    )
    query, key, value = (qkv[..., k * HEAD_DIM : (k + 1) * HEAD_DIM] for k in range(3))
    bias = lax.dynamic_slice_in_dim(gate_bias, head, 1, 1)
    decay = lax.dynamic_slice_in_dim(decay_shift, head, 1, 2)[..., 0]
    decay = jnp.concatenate([lax.dynamic_slice_in_dim(decay, k, 1, 0) for k in order], axis=0)
    entry = gates[:, 0] + bias[0]
    log_forget = jax.nn.log_sigmoid(gates[:, 1] + bias[1]) + decay
    sums = jnp.cumsum(log_forget, axis=-1)
    total = sums[:, -1]
    local_logs = total[:, None] - sums + entry
    peak = jnp.max(local_logs, axis=-1)
    scale = HEAD_DIM ** (-0.5)
    local_weights = jnp.exp(local_logs - peak[:, None]) * scale

    weighted = (local_weights[..., None] * value.astype(F32)).astype(BF16)
    state = dot(weighted, key, (((1,), (1,)), ((0,), (0,))))

    places = lax.axis_size(SP)
    cut = HEAD_DIM // places
    slices = state.astype(BF16).reshape(seqs, places, cut, HEAD_DIM).transpose(1, 0, 2, 3)
    slices = slices.reshape(places, seqs * cut, HEAD_DIM)
    numbers = thirds(jnp.stack([total, peak])).astype(BF16).reshape(1, 1, -1)
    count = numbers.shape[2]
    numbers = jnp.pad(numbers, ((0, 0), (0, seqs * cut - 1), (0, HEAD_DIM - count)))
    numbers = jnp.broadcast_to(numbers, slices.shape)
    packed = jnp.concatenate([slices, numbers], axis=1)
    everywhere = exchanged(packed, SP)
    found = everywhere[:, seqs * cut, :count].astype(F32).reshape(places, 3, 2, seqs)
    found = found[:, 0] + found[:, 1] + found[:, 2]
    totals, peaks = found[:, 0].T, found[:, 1].T
    line = jnp.arange(places)
    earlier = line[:, None] > line[None, :]
    masked = jnp.where(earlier, totals[:, None, :], 0.0)
    between = lax.dot_general(
        masked, earlier.astype(F32), (((2,), (0,)), ((), ())), precision=HIGHEST
    )
    since_start = jnp.sum(masked, axis=-1)
    logs = jnp.where(earlier, between + peaks[:, None, :], -jnp.inf)
    carried_peak = jnp.maximum(since_start, jnp.max(logs, axis=-1))
    mixing = jnp.exp(logs - carried_peak[..., None]).astype(BF16)
    states = everywhere[:, : seqs * cut].reshape(places, seqs, cut * HEAD_DIM)
    carried = dot(mixing, states, (((2,), (0,)), ((0,), (1,)))).astype(BF16)
    carried = carried.transpose(1, 0, 2).reshape(places, seqs * cut, HEAD_DIM)
    carried = exchanged(carried, SP)
    carried = carried.reshape(places, seqs, cut, HEAD_DIM).transpose(1, 0, 2, 3)
    prior_state = carried.reshape(seqs, HEAD_DIM, HEAD_DIM)
    place = lax.axis_index(SP)
    prior_peak = lax.dynamic_slice_in_dim(carried_peak, place, 1, 1)

    (conv,) = call(
        project_conv_kernel,
        [((seqs, tokens, 3 * channels), BF16)],
        spot,
        [*pieces, w_rest],
        10**9 * 3,
    )
    gate, mult, inlet = (conv[..., k * channels : (k + 1) * channels] for k in range(3))
    product = (mult.astype(F32) * inlet.astype(F32)).astype(BF16)
    taps = conv_taps.shape[0]
    rim = from_behind(product[:, tokens - (taps - 1) :], SP)
    padded = jnp.concatenate([rim, product], axis=1).astype(F32)
    tap_rows = lax.dynamic_slice_in_dim(conv_taps, head * channels, channels, 1)
    mixed = tap_rows[0] * padded[:, :tokens]
    for j in range(1, taps):
        mixed = mixed + tap_rows[j] * padded[:, j : j + tokens]
    conv_out = (gate.astype(F32) * mixed).astype(BF16)
    spans = jnp.arange(tokens)
    causal = spans[:, None] >= spans[None, :]
    pair_logs = jnp.where(
        causal, sums[:, :, None] - sums[:, None, :] + entry[:, None, :], -jnp.inf
    )
    carried_logs = sums + prior_peak
    row_peak = jnp.maximum(carried_logs, jnp.max(pair_logs, axis=-1))
    inner_weights = jnp.exp(pair_logs - row_peak[..., None]) * scale
    carried_weights = jnp.exp(carried_logs - row_peak)
    scores = inner_weights * dot(query, key, (((2,), (2,)), ((0,), (0,))))
    cell = carried_weights[..., None] * dot(query, prior_state, (((2,), (2,)), ((0,), (0,))))
    cell = cell + dot(scores.astype(BF16), value, (((2,), (1,)), ((0,), (0,))))
    cell = cell * lax.rsqrt(jnp.mean(cell * cell, axis=-1, keepdims=True) + EPSILON)
    gain = lax.dynamic_slice_in_dim(head_gain, head * HEAD_DIM, HEAD_DIM, 0)
    mem_out = (cell * gain).astype(BF16)
    both = rolled(jnp.concatenate([conv_out, mem_out], axis=-1), place_x)
    both = exchanged(both, "fs")
    (output,) = call(
        output_kernel, [((tokens, width), BF16)], spot, [both, *w_out], 10**9 * 2
    )

    cores = lax.axis_size("tp")
    parts = exchanged(output.reshape(cores, tokens // cores, width), "tp")
    return jnp.sum(parts.astype(F32), axis=0).astype(BF16)[None]


def solution(mesh):
    finer = Mesh(
        mesh.devices.reshape(8, 8, mesh.shape["fs"], mesh.shape["tp"]), ("sp_0", "sp_1", "fs", "tp")
    )
    weights = P(SP, ("fs", "tp"))
    return jax.shard_map(
        shards,
        mesh=finer,
        in_specs=(
            P("fs", SP, None),
            P(),
            weights,
            weights,
            weights,
            P(),
            weights,
            weights,
            weights,
            P(),
            P(),
            P(),
            P(None, SP, None),
            P(),
            P(("fs", "tp"), SP),
            P(("fs", "tp"), SP),
        ),
        out_specs=P("fs", SP_TP, None),
        check_vma=False,
    )
```

```python
import jax
import jax.numpy as jnp
from jax import lax
from jax.experimental import pallas as pl
from jax.experimental.pallas import tpu as pltpu
from jax.sharding import Mesh
from jax.sharding import PartitionSpec as P


HEAD_DIM = 128
Y = ("y_hi", "y_lo")
SP = ("z", *Y)
SP_TP = (*SP, "tp")
EPSILON = 1e-06
FAR_BELOW = -1e30
HIGHEST = lax.Precision.HIGHEST
F32 = jnp.float32
BF16 = jnp.bfloat16


def everyone(array, axis):
    copies = jnp.broadcast_to(array, (lax.axis_size(axis), *array.shape))
    return lax.all_to_all(copies, axis, split_axis=0, concat_axis=0, tiled=True)


def exchanged(array, axis):
    return lax.all_to_all(array, axis, split_axis=0, concat_axis=0, tiled=True)


def other_core(array):
    return lax.ppermute(array, "tp", [(0, 1), (1, 0)])


def from_behind(array, axis):
    peers = lax.axis_size(axis)
    return lax.ppermute(array, axis, [(i, i + 1) for i in range(peers - 1)])


def thirds(x):
    first = lax.reduce_precision(x, 8, 7)
    second = lax.reduce_precision(x - first, 8, 7)
    third = lax.reduce_precision(x - first - second, 8, 7)
    return jnp.stack([first, second, third])


def numbers_row(total, peak):
    numbers = thirds(jnp.stack([total, peak])).astype(BF16).reshape(1, -1)
    return jnp.pad(numbers, ((0, 0), (0, HEAD_DIM - numbers.shape[1])))


def numbers_of(rows, seqs):
    found = rows[:, : 6 * seqs].astype(F32).reshape(-1, 3, 2, seqs)
    found = found[:, 0] + found[:, 1] + found[:, 2]
    return found[:, 0].T, found[:, 1].T


def segment_logs(totals, peaks, earlier, after):
    masked = jnp.where(earlier, totals[:, None, :], 0.0)
    dims = (((2,), (0,)), ((), ()))
    between = lax.dot_general(masked, after, dims, precision=HIGHEST)
    logs = jnp.where(earlier, between + peaks[:, None, :], -jnp.inf)
    return jnp.sum(masked, axis=-1), logs


def dot(a, b, dims):
    return lax.dot_general(a, b, dims, preferred_element_type=F32)


def ring(array, axis, by):
    peers = lax.axis_size(axis)
    return lax.ppermute(array, axis, [(i, (i + by) % peers) for i in range(peers)])


def around(array, axis):
    return ring(array, axis, -1), ring(array, axis, 2), ring(array, axis, 1)


def relayed(array, axis):
    cut = array.shape[0] // 2
    ahead = ring(array, axis, -1)
    behind = ring(array, axis, 1)
    first = ring(behind[:cut], axis, 1)
    second = ring(ahead[cut:], axis, -1)
    return ahead, jnp.concatenate([first, second], axis=0), behind


def rolled(array, by):
    size = array.shape[0]
    twice = jnp.concatenate([array, array], axis=0)
    return lax.dynamic_slice_in_dim(twice, (size - by) % size, size, 0)


def matmuls(core, pieces, weights, left, out):
    half = pieces[0].shape[1]
    first = pl.multiple_of(core * half, half)
    second = pl.multiple_of((1 - core) * half, half)
    right = left + out.shape[2]
    for k in range(4):
        mixed = jnp.dot(
            pieces[2 * k][...],
            weights[pl.ds(first, half), left:right],
            preferred_element_type=F32,
        )
        mixed += jnp.dot(
            pieces[2 * k + 1][...],
            weights[pl.ds(second, half), left:right],
            preferred_element_type=F32,
        )
        out[k] = mixed.astype(BF16)


def project_mem_kernel(spot, *refs):
    parts, pieces, gate_rows = refs[:4], refs[4:12], refs[12]
    out, gates, weights = refs[13:]
    core = spot[0]
    for k in range(4):
        place = (spot[2] + k) % 4
        for z in range(8):
            start = pl.multiple_of((z * 4 + place) * 64, 64)
            weights[pl.ds(start, 64), :] = parts[k][pl.ds(z * 64, 64), :]
    matmuls(core, pieces, weights, 0, out)
    dims = (((1,), (1,)), ((), ()))
    for k in range(4):
        rows = dot(gate_rows[core], pieces[2 * k][...], dims)
        gates[k] = rows + dot(gate_rows[1 - core], pieces[2 * k + 1][...], dims)


def project_conv_kernel(spot, *refs):
    matmuls(spot[0], refs[:8], refs[8], 0, refs[9])


def output_kernel(spot, parts, *refs):
    weights, out = refs[:4], refs[4]
    dims = (((1,), (1,)), ((), ()))
    mixed = dot(parts[spot[1]], weights[0][...], dims)
    for k in range(1, 4):
        mixed += dot(parts[(spot[1] + k) % 4], weights[k][...], dims)
    out[...] = mixed.astype(BF16)


def in_vmem(count):
    return [pl.BlockSpec(memory_space=pltpu.VMEM)] * count


def call(kernel, shapes, spot, arrays, flops, scratch=()):
    smem = [pl.BlockSpec(memory_space=pltpu.SMEM)] if spot is not None else []
    return pl.pallas_call(
        kernel,
        out_shape=tuple(jax.ShapeDtypeStruct(shape, dtype) for shape, dtype in shapes),
        in_specs=smem + in_vmem(len(arrays)),
        out_specs=tuple(in_vmem(len(shapes))),
        scratch_shapes=list(scratch),
        cost_estimate=pl.CostEstimate(flops=flops, bytes_accessed=6 << 20, transcendentals=0),
    )(*([spot] if spot is not None else []), *arrays)


def shards(
    activations,
    norm_gain,
    w_conv_gate,
    w_conv_mult,
    w_conv_in,
    conv_taps,
    w_query,
    w_key,
    w_value,
    w_input_gate,
    w_forget_gate,
    gate_bias,
    decay_shift,
    head_gain,
    w_out_conv,
    w_out_mem,
):
    head = lax.axis_index("fs") * lax.axis_size("tp") + lax.axis_index("tp")
    core = lax.axis_index("tp")
    tokens, width = activations.shape[1:]
    half = width // 2
    seqs = lax.axis_size("fs")

    place_x = lax.axis_index("fs")
    order = [(place_x + by) % seqs for by in range(seqs)]

    place_y = lax.axis_index("y_hi")
    spot = jnp.stack([core, place_x, place_y]).astype(jnp.int32)

    channels = w_conv_gate.shape[1]
    w_rest = jnp.concatenate(
        [w_conv_gate, w_conv_mult, w_conv_in, w_out_conv.T, w_out_mem.T], axis=1
    )
    w_mem = jnp.concatenate([w_query, w_key, w_value], axis=1)
    w_rest, w_mem = lax.optimization_barrier((w_rest, w_mem))
    w_mem = everyone(w_mem, ("z", "y_lo")).reshape(-1, w_mem.shape[1])
    w_mem = (w_mem, *relayed(w_mem, "y_hi"))

    w_rest = lax.all_gather(w_rest, SP, axis=0, tiled=True)
    w_own = w_rest[:, 3 * channels :]
    w_out = (w_own, *relayed(w_own, "fs"))

    x = activations[0].astype(F32)
    normed = (
        x * lax.rsqrt(jnp.mean(x * x, axis=-1, keepdims=True) + EPSILON) * norm_gain
    ).astype(BF16)
    mine = lax.dynamic_slice_in_dim(normed, core * half, half, 1)
    pieces = [mine, lax.dynamic_slice_in_dim(normed, (1 - core) * half, half, 1)]
    others = around(mine, "fs")
    swapped = other_core(jnp.concatenate(others, axis=0))
    for k, piece in enumerate(others):
        pieces += [piece, swapped[k * tokens : (k + 1) * tokens]]

    gate_rows = jnp.concatenate(
        [
            lax.dynamic_slice_in_dim(w_input_gate, head, 1, 1),
            lax.dynamic_slice_in_dim(w_forget_gate, head, 1, 1),
        ],
        axis=1,
    ).T
    gate_rows = jnp.pad(gate_rows, ((0, 14), (0, 0))).reshape(16, 2, half).transpose(1, 0, 2)
    qkv, gates = call(
        project_mem_kernel,
        [((seqs, tokens, 3 * HEAD_DIM), BF16), ((seqs, 16, tokens), F32)],
        spot,
        [*w_mem, *pieces, gate_rows],
        10**9 * 3,
        [pltpu.VMEM((width, 3 * HEAD_DIM), BF16)],
    )
    query, key, value = (qkv[..., k * HEAD_DIM : (k + 1) * HEAD_DIM] for k in range(3))
    bias = lax.dynamic_slice_in_dim(gate_bias, head, 1, 1)
    decay = lax.dynamic_slice_in_dim(decay_shift, head, 1, 2)[..., 0]
    decay = jnp.concatenate([lax.dynamic_slice_in_dim(decay, k, 1, 0) for k in order], axis=0)
    entry = gates[:, 0] + bias[0]
    log_forget = jax.nn.log_sigmoid(gates[:, 1] + bias[1]) + decay
    sums = jnp.cumsum(log_forget, axis=-1)
    total = sums[:, -1]
    local_logs = total[:, None] - sums + entry
    peak = jnp.max(local_logs, axis=-1)
    scale = HEAD_DIM ** (-0.5)
    local_weights = jnp.exp(local_logs - peak[:, None]) * scale

    weighted = (local_weights[..., None] * value.astype(F32)).astype(BF16)
    state = dot(weighted, key, (((1,), (1,)), ((0,), (0,))))

    places = lax.axis_size(Y)
    cut = HEAD_DIM // places
    slices = state.astype(BF16).reshape(seqs, places, cut, HEAD_DIM).transpose(1, 0, 2, 3)
    slices = slices.reshape(places, seqs * cut, HEAD_DIM)
    numbers = jnp.broadcast_to(numbers_row(total, peak), (places, 16, HEAD_DIM))
    packed = jnp.concatenate([slices, numbers], axis=1)
    packed = exchanged(packed, Y)
    line = jnp.arange(places)
    after = (line[:, None] > line[None, :]).astype(F32)
    totals, peaks = numbers_of(packed[:, seqs * cut], seqs)
    states = packed[:, : seqs * cut].reshape(places, seqs, cut * HEAD_DIM)
    earlier = jnp.arange(places + 1)[:, None] > line[None, :]
    sums_in, logs = segment_logs(totals, peaks, earlier, after)
    peak_in = jnp.maximum(jnp.max(logs, axis=-1), FAR_BELOW)
    row_mixing = jnp.exp(logs[:, places] - peak_in[:, places, None])
    row_state = jnp.einsum("sj,jsk->sk", row_mixing.astype(BF16), states, preferred_element_type=F32)
    row_numbers = jnp.broadcast_to(
        numbers_row(sums_in[:, places], peak_in[:, places]), (16, HEAD_DIM)
    )
    row_packed = jnp.concatenate(
        [row_state.astype(BF16).reshape(seqs * cut, HEAD_DIM), row_numbers], axis=0
    )
    row_packed = everyone(row_packed, "z")
    row_totals, row_peaks = numbers_of(row_packed[:, seqs * cut], seqs)
    row_states = row_packed[:, : seqs * cut].reshape(places, seqs, cut * HEAD_DIM)
    earlier_rows = (line < lax.axis_index("z"))[None]
    before, row_logs = segment_logs(row_totals, row_peaks, earlier_rows, after)
    start_peak = jnp.maximum(before, jnp.max(row_logs, axis=-1))
    start_mixing = jnp.exp(row_logs - start_peak[..., None])[:, 0]
    start_state = jnp.einsum(
        "sj,jsk->sk", start_mixing.astype(BF16), row_states, preferred_element_type=F32
    )
    moved = sums_in[:, :places] + start_peak
    carried_peak = jnp.maximum(moved, peak_in[:, :places])
    mixing = jnp.exp(logs[:, :places] - carried_peak[..., None]).astype(BF16)
    carried = jnp.einsum("spj,jsk->spk", mixing, states, preferred_element_type=F32)
    carried = carried + jnp.exp(moved - carried_peak)[..., None] * start_state[:, None]
    carried = carried.astype(BF16).transpose(1, 0, 2).reshape(places, seqs * cut, HEAD_DIM)
    carried = exchanged(carried, Y)
    carried = carried.reshape(places, seqs, cut, HEAD_DIM).transpose(1, 0, 2, 3)
    prior_state = carried.reshape(seqs, HEAD_DIM, HEAD_DIM)
    prior_peak = lax.dynamic_slice_in_dim(carried_peak, lax.axis_index(Y), 1, 1)

    (conv,) = call(
        project_conv_kernel,
        [((seqs, tokens, 3 * channels), BF16)],
        spot,
        [*pieces, w_rest],
        10**9 * 3,
    )
    gate, mult, inlet = (conv[..., k * channels : (k + 1) * channels] for k in range(3))
    product = (mult.astype(F32) * inlet.astype(F32)).astype(BF16)
    taps = conv_taps.shape[0]
    rim = from_behind(product[:, tokens - (taps - 1) :], SP)
    padded = jnp.concatenate([rim, product], axis=1).astype(F32)
    tap_rows = lax.dynamic_slice_in_dim(conv_taps, head * channels, channels, 1)
    mixed = tap_rows[0] * padded[:, :tokens]
    for j in range(1, taps):
        mixed = mixed + tap_rows[j] * padded[:, j : j + tokens]
    conv_out = (gate.astype(F32) * mixed).astype(BF16)
    spans = jnp.arange(tokens)
    causal = spans[:, None] >= spans[None, :]
    pair_logs = jnp.where(
        causal, sums[:, :, None] - sums[:, None, :] + entry[:, None, :], -jnp.inf
    )
    carried_logs = sums + prior_peak
    row_peak = jnp.maximum(carried_logs, jnp.max(pair_logs, axis=-1))
    inner_weights = jnp.exp(pair_logs - row_peak[..., None]) * scale
    carried_weights = jnp.exp(carried_logs - row_peak)
    scores = inner_weights * dot(query, key, (((2,), (2,)), ((0,), (0,))))
    cell = carried_weights[..., None] * dot(query, prior_state, (((2,), (2,)), ((0,), (0,))))
    cell = cell + dot(scores.astype(BF16), value, (((2,), (1,)), ((0,), (0,))))
    cell = cell * lax.rsqrt(jnp.mean(cell * cell, axis=-1, keepdims=True) + EPSILON)
    gain = lax.dynamic_slice_in_dim(head_gain, head * HEAD_DIM, HEAD_DIM, 0)
    mem_out = (cell * gain).astype(BF16)
    both = rolled(jnp.concatenate([conv_out, mem_out], axis=-1), place_x)
    both = exchanged(both, "fs")
    (output,) = call(
        output_kernel, [((tokens, width), BF16)], spot, [both, *w_out], 10**9 * 2
    )

    cores = lax.axis_size("tp")
    parts = exchanged(output.reshape(cores, tokens // cores, width), "tp")
    return jnp.sum(parts.astype(F32), axis=0).astype(BF16)[None]


def solution(mesh):
    sizes = (8, 4, 2, mesh.shape["fs"], mesh.shape["tp"])
    finer = Mesh(mesh.devices.reshape(sizes), (*SP, "fs", "tp"))
    weights = P(SP, ("fs", "tp"))
    return jax.shard_map(
        shards,
        mesh=finer,
        in_specs=(
            P("fs", SP, None),
            P(),
            weights,
            weights,
            weights,
            P(),
            weights,
            weights,
            weights,
            P(),
            P(),
            P(),
            P(None, SP, None),
            P(),
            P(("fs", "tp"), SP),
            P(("fs", "tp"), SP),
        ),
        out_specs=P("fs", SP_TP, None),
        check_vma=False,
    )
```

```python
import jax
import jax.numpy as jnp
from jax import lax
from jax.experimental import pallas as pl
from jax.experimental.pallas import tpu as pltpu
from jax.sharding import Mesh
from jax.sharding import PartitionSpec as P


HEAD_DIM = 128
Y = ("y_hi", "y_lo")
SP = ("z", *Y)
SP_TP = (*SP, "tp")
EPSILON = 1e-06
FAR_BELOW = -1e30
HIGHEST = lax.Precision.HIGHEST
F32 = jnp.float32
BF16 = jnp.bfloat16


def everyone(array, axis):
    copies = jnp.broadcast_to(array, (lax.axis_size(axis), *array.shape))
    return lax.all_to_all(copies, axis, split_axis=0, concat_axis=0, tiled=True)


def exchanged(array, axis):
    return lax.all_to_all(array, axis, split_axis=0, concat_axis=0, tiled=True)


def other_core(array):
    return lax.ppermute(array, "tp", [(0, 1), (1, 0)])


def from_behind(array, axis):
    peers = lax.axis_size(axis)
    return lax.ppermute(array, axis, [(i, i + 1) for i in range(peers - 1)])


def thirds(x):
    first = lax.reduce_precision(x, 8, 7)
    second = lax.reduce_precision(x - first, 8, 7)
    third = lax.reduce_precision(x - first - second, 8, 7)
    return jnp.stack([first, second, third])


def numbers_row(total, peak):
    numbers = thirds(jnp.stack([total, peak])).astype(BF16).reshape(1, -1)
    return jnp.pad(numbers, ((0, 0), (0, HEAD_DIM - numbers.shape[1])))


def numbers_of(rows, seqs):
    found = rows[:, : 6 * seqs].astype(F32).reshape(-1, 3, 2, seqs)
    found = found[:, 0] + found[:, 1] + found[:, 2]
    return found[:, 0].T, found[:, 1].T


def segment_logs(totals, peaks, earlier, after):
    masked = jnp.where(earlier, totals[:, None, :], 0.0)
    dims = (((2,), (0,)), ((), ()))
    between = lax.dot_general(masked, after, dims, precision=HIGHEST)
    logs = jnp.where(earlier, between + peaks[:, None, :], -jnp.inf)
    return jnp.sum(masked, axis=-1), logs


def dot(a, b, dims):
    return lax.dot_general(a, b, dims, preferred_element_type=F32)


def ring(array, axis, by):
    peers = lax.axis_size(axis)
    return lax.ppermute(array, axis, [(i, (i + by) % peers) for i in range(peers)])


def around(array, axis):
    return ring(array, axis, -1), ring(array, axis, 2), ring(array, axis, 1)


def relayed(array, axis):
    cut = array.shape[0] // 2
    ahead = ring(array, axis, -1)
    behind = ring(array, axis, 1)
    first = ring(behind[:cut], axis, 1)
    second = ring(ahead[cut:], axis, -1)
    return ahead, first, second, behind


def rolled(array, by):
    size = array.shape[0]
    twice = jnp.concatenate([array, array], axis=0)
    return lax.dynamic_slice_in_dim(twice, (size - by) % size, size, 0)


def pack_kernel(*refs):
    parts, rest, mem = refs[:8], refs[8], refs[9]
    wide = parts[0].shape[1]
    for k in range(3):
        for copy in range(mem.shape[0]):
            mem[copy, :, k * wide : (k + 1) * wide] = parts[k][...]
    for k in range(5):
        rest[:, k * wide : (k + 1) * wide] = parts[3 + k][...]


def piece(refs, k, other):
    tokens = refs[0].shape[0]
    if k == 0:
        return refs[other][...]
    if other:
        return refs[5][(k - 1) * tokens : k * tokens, :]
    return refs[1 + k][...]


def matmul(core, pieces, weights, k, out):
    half = pieces[0].shape[1]
    first = pl.multiple_of(core * half, half)
    second = pl.multiple_of((1 - core) * half, half)
    wide = out.shape[2]
    mixed = jnp.dot(
        piece(pieces, k, 0), weights[pl.ds(first, half), :wide], preferred_element_type=F32
    )
    mixed += jnp.dot(
        piece(pieces, k, 1), weights[pl.ds(second, half), :wide], preferred_element_type=F32
    )
    out[k] = mixed.astype(BF16)


def project_mem_kernel(spot, bias, *refs):
    parts, pieces, gate_rows, decay = refs[:5], refs[5:11], refs[11], refs[12]
    out, packed, sums_out, entry_out, weights = refs[13:]
    core = spot[0]
    for k, sources in enumerate(((0, 0), (1, 1), (2, 3), (4, 4))):
        place = (spot[2] + k) % 4
        for z in range(8):
            start = pl.multiple_of((z * 4 + place) * 64, 64)
            source = parts[sources[z // 4]]
            row = (z * 64) % source.shape[0]
            weights[pl.ds(start, 64), :] = source[row : row + 64, :]
    dims = (((1,), (1,)), ((), ()))
    gates = [
        dot(gate_rows[core], piece(pieces, k, 0), dims)
        + dot(gate_rows[1 - core], piece(pieces, k, 1), dims)
        for k in range(4)
    ]
    entry = jnp.concatenate([g[0:1] for g in gates], axis=0) + bias[0]
    forget = jnp.concatenate([g[1:2] for g in gates], axis=0) + bias[1]
    small = jnp.exp(-jnp.abs(forget))
    series = small * (1.0 - small * (0.5 - small * (1.0 / 3.0)))
    softened = jnp.where(small < 1e-3, series, jnp.log(1.0 + small))
    log_forget = jnp.minimum(forget, 0.0) - softened + decay[...]
    tokens = entry.shape[1]
    shape = (tokens, tokens)
    upto = lax.broadcasted_iota(jnp.int32, shape, 0) <= lax.broadcasted_iota(jnp.int32, shape, 1)
    sums = jnp.dot(
        log_forget, upto.astype(F32), preferred_element_type=F32, precision=HIGHEST
    )
    sums_out[...] = sums
    entry_out[...] = entry
    total = sums[:, tokens - 1 :]
    local_logs = total - sums + entry
    peak = jnp.max(local_logs, axis=1, keepdims=True)
    local_weights = jnp.exp(local_logs - peak) * HEAD_DIM ** (-0.5)
    columns = jnp.concatenate([local_weights, local_weights], axis=0).T
    for k in range(4):
        matmul(core, pieces, weights, k, out)
        value = out[k, :, 2 * HEAD_DIM :].astype(F32)
        weighted = (value * columns[:, k : k + 1]).astype(BF16)
        state = dot(weighted, out[k, :, HEAD_DIM : 2 * HEAD_DIM], (((0,), (0,)), ((), ())))
        state = state.astype(BF16)
        for c in range(8):
            packed[c, k * 16 : (k + 1) * 16, :] = state[c * 16 : (c + 1) * 16, :]
    numbers = jnp.concatenate([total, peak], axis=0)
    first = numbers.astype(BF16).astype(F32)
    second = (numbers - first).astype(BF16).astype(F32)
    third = numbers - first - second
    numbers = jnp.concatenate([first, second, third, third], axis=0)
    numbers = jnp.broadcast_to(numbers, (32, HEAD_DIM)).astype(BF16)
    for c in range(8):
        packed[c, 64:96, :] = numbers


def project_conv_kernel(spot, *refs):
    for k in range(4):
        matmul(spot[0], refs[:6], refs[6], k, refs[7])


def output_kernel(spot, parts, own, ahead, first, second, behind, out):
    dims = (((1,), (1,)), ((), ()))
    half = first.shape[0]
    for side, far in enumerate((first, second)):
        rows = slice(side * half, (side + 1) * half)
        mixed = dot(parts[spot[1]], own[rows, :], dims)
        mixed += dot(parts[(spot[1] + 1) % 4], ahead[rows, :], dims)
        mixed += dot(parts[(spot[1] + 2) % 4], far[...], dims)
        mixed += dot(parts[(spot[1] + 3) % 4], behind[rows, :], dims)
        out[:, rows] = mixed.astype(BF16)


def in_vmem(count):
    return [pl.BlockSpec(memory_space=pltpu.VMEM)] * count


def call(kernel, shapes, scalars, arrays, flops, scratch=()):
    return pl.pallas_call(
        kernel,
        out_shape=tuple(jax.ShapeDtypeStruct(shape, dtype) for shape, dtype in shapes),
        in_specs=[pl.BlockSpec(memory_space=pltpu.SMEM)] * len(scalars) + in_vmem(len(arrays)),
        out_specs=tuple(in_vmem(len(shapes))),
        scratch_shapes=list(scratch),
        cost_estimate=pl.CostEstimate(flops=flops, bytes_accessed=6 << 20, transcendentals=0),
    )(*scalars, *arrays)


def shards(
    activations,
    norm_gain,
    w_conv_gate,
    w_conv_mult,
    w_conv_in,
    conv_taps,
    w_query,
    w_key,
    w_value,
    w_input_gate,
    w_forget_gate,
    gate_bias,
    decay_shift,
    head_gain,
    w_out_conv,
    w_out_mem,
):
    head = lax.axis_index("fs") * lax.axis_size("tp") + lax.axis_index("tp")
    core = lax.axis_index("tp")
    tokens, width = activations.shape[1:]
    half = width // 2
    seqs = lax.axis_size("fs")

    place_x = lax.axis_index("fs")
    order = [(place_x + by) % seqs for by in range(seqs)]

    place_y = lax.axis_index("y_hi")
    spot = jnp.stack([core, place_x, place_y]).astype(jnp.int32)

    channels = w_conv_gate.shape[1]
    shard = w_query.shape
    pairs = 2 * lax.axis_size("z")
    w_rest, w_mem = call(
        pack_kernel,
        [((shard[0], 5 * shard[1]), BF16), ((pairs, shard[0], 3 * shard[1]), BF16)],
        [],
        [w_query, w_key, w_value, w_conv_gate, w_conv_mult, w_conv_in, w_out_conv.T, w_out_mem.T],
        10**6,
    )
    w_mem = exchanged(w_mem, ("z", "y_lo")).reshape(-1, w_mem.shape[2])
    w_mem = (w_mem, *relayed(w_mem, "y_hi"))

    w_rest = lax.all_gather(w_rest, SP, axis=0, tiled=True)
    w_own = w_rest[:, 3 * channels :]
    w_out = (w_own, *relayed(w_own, "fs"))

    x = activations[0].astype(F32)
    normed = (
        x * lax.rsqrt(jnp.mean(x * x, axis=-1, keepdims=True) + EPSILON) * norm_gain
    ).astype(BF16)
    mine = lax.dynamic_slice_in_dim(normed, core * half, half, 1)
    pieces = [mine, lax.dynamic_slice_in_dim(normed, (1 - core) * half, half, 1)]
    others = around(mine, "fs")
    together = jnp.concatenate(others, axis=0)
    swapped = other_core(together)
    pieces += [*others, swapped]

    gate_rows = jnp.concatenate(
        [
            lax.dynamic_slice_in_dim(w_input_gate, head, 1, 1),
            lax.dynamic_slice_in_dim(w_forget_gate, head, 1, 1),
        ],
        axis=1,
    ).T
    gate_rows = jnp.pad(gate_rows, ((0, 14), (0, 0))).reshape(16, 2, half).transpose(1, 0, 2)
    bias = lax.dynamic_slice_in_dim(gate_bias, head, 1, 1)[:, 0]
    decay = lax.dynamic_slice_in_dim(decay_shift, head, 1, 2)[..., 0]
    decay = jnp.concatenate([lax.dynamic_slice_in_dim(decay, k, 1, 0) for k in order], axis=0)
    places = lax.axis_size(Y)
    cut = HEAD_DIM // places
    qkv, packed, sums, entry = call(
        project_mem_kernel,
        [
            ((seqs, tokens, 3 * HEAD_DIM), BF16),
            ((places, seqs * cut + 32, HEAD_DIM), BF16),
            ((seqs, tokens), F32),
            ((seqs, tokens), F32),
        ],
        [spot, bias],
        [*w_mem, *pieces, gate_rows, decay],
        10**9 * 3,
        [pltpu.VMEM((width, 3 * HEAD_DIM), BF16)],
    )
    query, key, value = (qkv[..., k * HEAD_DIM : (k + 1) * HEAD_DIM] for k in range(3))
    scale = HEAD_DIM ** (-0.5)

    packed = exchanged(packed, Y)
    line = jnp.arange(places)
    after = (line[:, None] > line[None, :]).astype(F32)
    totals, peaks = numbers_of(packed[:, seqs * cut :, 0], seqs)
    states = packed[:, : seqs * cut].reshape(places, seqs, cut * HEAD_DIM)
    earlier = jnp.arange(places + 1)[:, None] > line[None, :]
    sums_in, logs = segment_logs(totals, peaks, earlier, after)
    peak_in = jnp.maximum(jnp.max(logs, axis=-1), FAR_BELOW)
    row_mixing = jnp.exp(logs[:, places] - peak_in[:, places, None])
    row_state = jnp.einsum("sj,jsk->sk", row_mixing.astype(BF16), states, preferred_element_type=F32)
    row_numbers = jnp.broadcast_to(
        numbers_row(sums_in[:, places], peak_in[:, places]), (16, HEAD_DIM)
    )
    row_packed = jnp.concatenate(
        [row_state.astype(BF16).reshape(seqs * cut, HEAD_DIM), row_numbers], axis=0
    )
    row_packed = everyone(row_packed, "z")
    row_totals, row_peaks = numbers_of(row_packed[:, seqs * cut], seqs)
    row_states = row_packed[:, : seqs * cut].reshape(places, seqs, cut * HEAD_DIM)
    earlier_rows = (line < lax.axis_index("z"))[None]
    before, row_logs = segment_logs(row_totals, row_peaks, earlier_rows, after)
    start_peak = jnp.maximum(before, jnp.max(row_logs, axis=-1))
    start_mixing = jnp.exp(row_logs - start_peak[..., None])[:, 0]
    start_state = jnp.einsum(
        "sj,jsk->sk", start_mixing.astype(BF16), row_states, preferred_element_type=F32
    )
    moved = sums_in[:, :places] + start_peak
    carried_peak = jnp.maximum(moved, peak_in[:, :places])
    mixing = jnp.exp(logs[:, :places] - carried_peak[..., None]).astype(BF16)
    carried = jnp.einsum("spj,jsk->spk", mixing, states, preferred_element_type=F32)
    carried = carried + jnp.exp(moved - carried_peak)[..., None] * start_state[:, None]
    carried = carried.astype(BF16).transpose(1, 0, 2).reshape(places, seqs * cut, HEAD_DIM)
    carried = exchanged(carried, Y)
    carried = carried.reshape(places, seqs, cut, HEAD_DIM).transpose(1, 0, 2, 3)
    prior_state = carried.reshape(seqs, HEAD_DIM, HEAD_DIM)
    prior_peak = lax.dynamic_slice_in_dim(carried_peak, lax.axis_index(Y), 1, 1)

    (conv,) = call(
        project_conv_kernel,
        [((seqs, tokens, 3 * channels), BF16)],
        [spot],
        [*pieces, w_rest],
        10**9 * 3,
    )
    gate, mult, inlet = (conv[..., k * channels : (k + 1) * channels] for k in range(3))
    product = (mult.astype(F32) * inlet.astype(F32)).astype(BF16)
    taps = conv_taps.shape[0]
    rim = from_behind(product[:, tokens - (taps - 1) :], SP)
    padded = jnp.concatenate([rim, product], axis=1).astype(F32)
    tap_rows = lax.dynamic_slice_in_dim(conv_taps, head * channels, channels, 1)
    mixed = tap_rows[0] * padded[:, :tokens]
    for j in range(1, taps):
        mixed = mixed + tap_rows[j] * padded[:, j : j + tokens]
    conv_out = (gate.astype(F32) * mixed).astype(BF16)
    spans = jnp.arange(tokens)
    causal = spans[:, None] >= spans[None, :]
    pair_logs = jnp.where(
        causal, sums[:, :, None] - sums[:, None, :] + entry[:, None, :], -jnp.inf
    )
    carried_logs = sums + prior_peak
    row_peak = jnp.maximum(carried_logs, jnp.max(pair_logs, axis=-1))
    inner_weights = jnp.exp(pair_logs - row_peak[..., None]) * scale
    carried_weights = jnp.exp(carried_logs - row_peak)
    scores = inner_weights * dot(query, key, (((2,), (2,)), ((0,), (0,))))
    cell = carried_weights[..., None] * dot(query, prior_state, (((2,), (2,)), ((0,), (0,))))
    cell = cell + dot(scores.astype(BF16), value, (((2,), (1,)), ((0,), (0,))))
    cell = cell * lax.rsqrt(jnp.mean(cell * cell, axis=-1, keepdims=True) + EPSILON)
    gain = lax.dynamic_slice_in_dim(head_gain, head * HEAD_DIM, HEAD_DIM, 0)
    mem_out = (cell * gain).astype(BF16)
    both = rolled(jnp.concatenate([conv_out, mem_out], axis=-1), place_x)
    both = exchanged(both, "fs")
    (output,) = call(output_kernel, [((tokens, width), BF16)], [spot], [both, *w_out], 10**9 * 2)

    cores = lax.axis_size("tp")
    parts = exchanged(output.reshape(cores, tokens // cores, width), "tp")
    return jnp.sum(parts.astype(F32), axis=0).astype(BF16)[None]


def solution(mesh):
    sizes = (8, 4, 2, mesh.shape["fs"], mesh.shape["tp"])
    finer = Mesh(mesh.devices.reshape(sizes), (*SP, "fs", "tp"))
    weights = P(SP, ("fs", "tp"))
    return jax.shard_map(
        shards,
        mesh=finer,
        in_specs=(
            P("fs", SP, None),
            P(),
            weights,
            weights,
            weights,
            P(),
            weights,
            weights,
            weights,
            P(),
            P(),
            P(),
            P(None, SP, None),
            P(),
            P(("fs", "tp"), SP),
            P(("fs", "tp"), SP),
        ),
        out_specs=P("fs", SP_TP, None),
        check_vma=False,
    )
```

```python
import jax
import jax.numpy as jnp
from jax import lax
from jax.experimental import pallas as pl
from jax.experimental.pallas import tpu as pltpu
from jax.sharding import Mesh
from jax.sharding import PartitionSpec as P


HEAD_DIM = 128
Y = ("y_hi", "y_lo")
SP = ("z", *Y)
SP_TP = (*SP, "tp")
EPSILON = 1e-06
FAR_BELOW = -1e30
HIGHEST = lax.Precision.HIGHEST
F32 = jnp.float32
BF16 = jnp.bfloat16


def everyone(array, axis):
    copies = jnp.broadcast_to(array, (lax.axis_size(axis), *array.shape))
    return lax.all_to_all(copies, axis, split_axis=0, concat_axis=0, tiled=True)


def exchanged(array, axis):
    return lax.all_to_all(array, axis, split_axis=0, concat_axis=0, tiled=True)


def other_core(array):
    return lax.ppermute(array, "tp", [(0, 1), (1, 0)])


def from_behind(array, axis):
    peers = lax.axis_size(axis)
    return lax.ppermute(array, axis, [(i, i + 1) for i in range(peers - 1)])


def thirds(x):
    first = lax.reduce_precision(x, 8, 7)
    second = lax.reduce_precision(x - first, 8, 7)
    third = lax.reduce_precision(x - first - second, 8, 7)
    return jnp.stack([first, second, third])


def numbers_row(total, peak):
    numbers = thirds(jnp.stack([total, peak])).astype(BF16).reshape(1, -1)
    return jnp.pad(numbers, ((0, 0), (0, HEAD_DIM - numbers.shape[1])))


def numbers_of(rows, seqs):
    found = rows[:, : 6 * seqs].astype(F32).reshape(-1, 3, 2, seqs)
    found = found[:, 0] + found[:, 1] + found[:, 2]
    return found[:, 0].T, found[:, 1].T


def segment_logs(totals, peaks, earlier, after):
    masked = jnp.where(earlier, totals[:, None, :], 0.0)
    dims = (((2,), (0,)), ((), ()))
    between = lax.dot_general(masked, after, dims, precision=HIGHEST)
    logs = jnp.where(earlier, between + peaks[:, None, :], -jnp.inf)
    return jnp.sum(masked, axis=-1), logs


def dot(a, b, dims):
    return lax.dot_general(a, b, dims, preferred_element_type=F32)


def ring(array, axis, by):
    peers = lax.axis_size(axis)
    return lax.ppermute(array, axis, [(i, (i + by) % peers) for i in range(peers)])


def around(array, axis):
    return ring(array, axis, -1), ring(array, axis, 2), ring(array, axis, 1)


def relayed(array, axis):
    cut = array.shape[0] // 2
    ahead = ring(array, axis, -1)
    behind = ring(array, axis, 1)
    first = ring(behind[:cut], axis, 1)
    second = ring(ahead[cut:], axis, -1)
    return ahead, first, second, behind


def rolled(array, by):
    size = array.shape[0]
    twice = jnp.concatenate([array, array], axis=0)
    return lax.dynamic_slice_in_dim(twice, (size - by) % size, size, 0)


def pack_kernel(*refs):
    parts, rest, mem = refs[:8], refs[8], refs[9]
    wide = parts[0].shape[1]
    for k in range(3):
        for copy in range(mem.shape[0]):
            mem[copy, :, k * wide : (k + 1) * wide] = parts[k][...]
    for k in range(5):
        for copy in range(rest.shape[0]):
            rest[copy, :, k * wide : (k + 1) * wide] = parts[3 + k][...]


def piece(refs, k, other):
    tokens = refs[0].shape[0]
    if k == 0:
        return refs[other][...]
    if other:
        return refs[5][(k - 1) * tokens : k * tokens, :]
    return refs[1 + k][...]


def matmul(core, pieces, weights, k, out):
    half = pieces[0].shape[1]
    first = pl.multiple_of(core * half, half)
    second = pl.multiple_of((1 - core) * half, half)
    wide = out.shape[2]
    mixed = jnp.dot(
        piece(pieces, k, 0), weights[pl.ds(first, half), :wide], preferred_element_type=F32
    )
    mixed += jnp.dot(
        piece(pieces, k, 1), weights[pl.ds(second, half), :wide], preferred_element_type=F32
    )
    out[k] = mixed.astype(BF16)


def project_mem_kernel(spot, bias, *refs):
    parts, pieces, gate_rows, decay = refs[:5], refs[5:11], refs[11], refs[12]
    out, packed, sums_out, entry_out, weights = refs[13:]
    core = spot[0]
    for k, sources in enumerate(((0, 0), (1, 1), (2, 3), (4, 4))):
        place = (spot[2] + k) % 4
        for z in range(8):
            start = pl.multiple_of((z * 4 + place) * 64, 64)
            source = parts[sources[z // 4]]
            row = (z * 64) % source.shape[0]
            weights[pl.ds(start, 64), :] = source[row : row + 64, :]
    dims = (((1,), (1,)), ((), ()))
    gates = [
        dot(gate_rows[core], piece(pieces, k, 0), dims)
        + dot(gate_rows[1 - core], piece(pieces, k, 1), dims)
        for k in range(4)
    ]
    entry = jnp.concatenate([g[0:1] for g in gates], axis=0) + bias[0]
    forget = jnp.concatenate([g[1:2] for g in gates], axis=0) + bias[1]
    small = jnp.exp(-jnp.abs(forget))
    series = small * (1.0 - small * (0.5 - small * (1.0 / 3.0)))
    softened = jnp.where(small < 1e-3, series, jnp.log(1.0 + small))
    log_forget = jnp.minimum(forget, 0.0) - softened + decay[...]
    tokens = entry.shape[1]
    shape = (tokens, tokens)
    upto = lax.broadcasted_iota(jnp.int32, shape, 0) <= lax.broadcasted_iota(jnp.int32, shape, 1)
    sums = jnp.dot(
        log_forget, upto.astype(F32), preferred_element_type=F32, precision=HIGHEST
    )
    sums_out[...] = sums
    entry_out[...] = entry
    total = sums[:, tokens - 1 :]
    local_logs = total - sums + entry
    peak = jnp.max(local_logs, axis=1, keepdims=True)
    local_weights = jnp.exp(local_logs - peak) * HEAD_DIM ** (-0.5)
    columns = jnp.concatenate([local_weights, local_weights], axis=0).T
    for k in range(4):
        matmul(core, pieces, weights, k, out)
        value = out[k, :, 2 * HEAD_DIM :].astype(F32)
        weighted = (value * columns[:, k : k + 1]).astype(BF16)
        state = dot(weighted, out[k, :, HEAD_DIM : 2 * HEAD_DIM], (((0,), (0,)), ((), ())))
        state = state.astype(BF16)
        for c in range(8):
            packed[c, k * 16 : (k + 1) * 16, :] = state[c * 16 : (c + 1) * 16, :]
    numbers = jnp.concatenate([total, peak], axis=0)
    first = numbers.astype(BF16).astype(F32)
    second = (numbers - first).astype(BF16).astype(F32)
    third = numbers - first - second
    numbers = jnp.concatenate([first, second, third, third], axis=0)
    numbers = jnp.broadcast_to(numbers, (32, HEAD_DIM)).astype(BF16)
    for c in range(8):
        packed[c, 64:96, :] = numbers


def project_conv_kernel(spot, *refs):
    for k in range(4):
        matmul(spot[0], refs[:6], refs[6], k, refs[7])


def output_kernel(spot, parts, own, ahead, first, second, behind, out):
    dims = (((1,), (1,)), ((), ()))
    half = first.shape[0]
    for side, far in enumerate((first, second)):
        rows = slice(side * half, (side + 1) * half)
        mixed = dot(parts[spot[1]], own[rows, :], dims)
        mixed += dot(parts[(spot[1] + 1) % 4], ahead[rows, :], dims)
        mixed += dot(parts[(spot[1] + 2) % 4], far[...], dims)
        mixed += dot(parts[(spot[1] + 3) % 4], behind[rows, :], dims)
        out[:, rows] = mixed.astype(BF16)


def in_vmem(count):
    return [pl.BlockSpec(memory_space=pltpu.VMEM)] * count


def call(kernel, shapes, scalars, arrays, flops, scratch=()):
    return pl.pallas_call(
        kernel,
        out_shape=tuple(jax.ShapeDtypeStruct(shape, dtype) for shape, dtype in shapes),
        in_specs=[pl.BlockSpec(memory_space=pltpu.SMEM)] * len(scalars) + in_vmem(len(arrays)),
        out_specs=tuple(in_vmem(len(shapes))),
        scratch_shapes=list(scratch),
        cost_estimate=pl.CostEstimate(flops=flops, bytes_accessed=6 << 20, transcendentals=0),
    )(*scalars, *arrays)


def shards(
    activations,
    norm_gain,
    w_conv_gate,
    w_conv_mult,
    w_conv_in,
    conv_taps,
    w_query,
    w_key,
    w_value,
    w_input_gate,
    w_forget_gate,
    gate_bias,
    decay_shift,
    head_gain,
    w_out_conv,
    w_out_mem,
):
    head = lax.axis_index("fs") * lax.axis_size("tp") + lax.axis_index("tp")
    core = lax.axis_index("tp")
    tokens, width = activations.shape[1:]
    half = width // 2
    seqs = lax.axis_size("fs")

    place_x = lax.axis_index("fs")
    order = [(place_x + by) % seqs for by in range(seqs)]

    place_y = lax.axis_index("y_hi")
    spot = jnp.stack([core, place_x, place_y]).astype(jnp.int32)

    channels = w_conv_gate.shape[1]
    shard = w_query.shape
    places = lax.axis_size(Y)
    pairs = 2 * lax.axis_size("z")
    w_rest, w_mem = call(
        pack_kernel,
        [((places, shard[0], 5 * shard[1]), BF16), ((pairs, shard[0], 3 * shard[1]), BF16)],
        [],
        [w_query, w_key, w_value, w_conv_gate, w_conv_mult, w_conv_in, w_out_conv.T, w_out_mem.T],
        10**6,
    )
    w_mem = exchanged(w_mem, ("z", "y_lo")).reshape(-1, w_mem.shape[2])
    w_mem = (w_mem, *relayed(w_mem, "y_hi"))

    w_rest = exchanged(w_rest, Y).reshape(-1, w_rest.shape[2])
    w_rest = lax.all_gather(w_rest, "z", axis=0, tiled=True)
    w_own = w_rest[:, 3 * channels :]
    w_out = (w_own, *relayed(w_own, "fs"))

    x = activations[0].astype(F32)
    normed = (
        x * lax.rsqrt(jnp.mean(x * x, axis=-1, keepdims=True) + EPSILON) * norm_gain
    ).astype(BF16)
    mine = lax.dynamic_slice_in_dim(normed, core * half, half, 1)
    pieces = [mine, lax.dynamic_slice_in_dim(normed, (1 - core) * half, half, 1)]
    others = around(mine, "fs")
    together = jnp.concatenate(others, axis=0)
    swapped = other_core(together)
    pieces += [*others, swapped]

    gate_rows = jnp.concatenate(
        [
            lax.dynamic_slice_in_dim(w_input_gate, head, 1, 1),
            lax.dynamic_slice_in_dim(w_forget_gate, head, 1, 1),
        ],
        axis=1,
    ).T
    gate_rows = jnp.pad(gate_rows, ((0, 14), (0, 0))).reshape(16, 2, half).transpose(1, 0, 2)
    bias = lax.dynamic_slice_in_dim(gate_bias, head, 1, 1)[:, 0]
    decay = lax.dynamic_slice_in_dim(decay_shift, head, 1, 2)[..., 0]
    decay = jnp.concatenate([lax.dynamic_slice_in_dim(decay, k, 1, 0) for k in order], axis=0)
    places = lax.axis_size(Y)
    cut = HEAD_DIM // places
    qkv, packed, sums, entry = call(
        project_mem_kernel,
        [
            ((seqs, tokens, 3 * HEAD_DIM), BF16),
            ((places, seqs * cut + 32, HEAD_DIM), BF16),
            ((seqs, tokens), F32),
            ((seqs, tokens), F32),
        ],
        [spot, bias],
        [*w_mem, *pieces, gate_rows, decay],
        10**9 * 3,
        [pltpu.VMEM((width, 3 * HEAD_DIM), BF16)],
    )
    query, key, value = (qkv[..., k * HEAD_DIM : (k + 1) * HEAD_DIM] for k in range(3))
    scale = HEAD_DIM ** (-0.5)

    packed = exchanged(packed, Y)
    line = jnp.arange(places)
    after = (line[:, None] > line[None, :]).astype(F32)
    totals, peaks = numbers_of(packed[:, seqs * cut :, 0], seqs)
    states = packed[:, : seqs * cut].reshape(places, seqs, cut * HEAD_DIM)
    earlier = jnp.arange(places + 1)[:, None] > line[None, :]
    sums_in, logs = segment_logs(totals, peaks, earlier, after)
    peak_in = jnp.maximum(jnp.max(logs, axis=-1), FAR_BELOW)
    row_mixing = jnp.exp(logs[:, places] - peak_in[:, places, None])
    row_state = jnp.einsum("sj,jsk->sk", row_mixing.astype(BF16), states, preferred_element_type=F32)
    row_numbers = jnp.broadcast_to(
        numbers_row(sums_in[:, places], peak_in[:, places]), (16, HEAD_DIM)
    )
    row_packed = jnp.concatenate(
        [row_state.astype(BF16).reshape(seqs * cut, HEAD_DIM), row_numbers], axis=0
    )
    row_packed = everyone(row_packed, "z")
    row_totals, row_peaks = numbers_of(row_packed[:, seqs * cut], seqs)
    row_states = row_packed[:, : seqs * cut].reshape(places, seqs, cut * HEAD_DIM)
    earlier_rows = (line < lax.axis_index("z"))[None]
    before, row_logs = segment_logs(row_totals, row_peaks, earlier_rows, after)
    start_peak = jnp.maximum(before, jnp.max(row_logs, axis=-1))
    start_mixing = jnp.exp(row_logs - start_peak[..., None])[:, 0]
    start_state = jnp.einsum(
        "sj,jsk->sk", start_mixing.astype(BF16), row_states, preferred_element_type=F32
    )
    moved = sums_in[:, :places] + start_peak
    carried_peak = jnp.maximum(moved, peak_in[:, :places])
    mixing = jnp.exp(logs[:, :places] - carried_peak[..., None]).astype(BF16)
    carried = jnp.einsum("spj,jsk->spk", mixing, states, preferred_element_type=F32)
    carried = carried + jnp.exp(moved - carried_peak)[..., None] * start_state[:, None]
    carried = carried.astype(BF16).transpose(1, 0, 2).reshape(places, seqs * cut, HEAD_DIM)
    carried = exchanged(carried, Y)
    carried = carried.reshape(places, seqs, cut, HEAD_DIM).transpose(1, 0, 2, 3)
    prior_state = carried.reshape(seqs, HEAD_DIM, HEAD_DIM)
    prior_peak = lax.dynamic_slice_in_dim(carried_peak, lax.axis_index(Y), 1, 1)

    (conv,) = call(
        project_conv_kernel,
        [((seqs, tokens, 3 * channels), BF16)],
        [spot],
        [*pieces, w_rest],
        10**9 * 3,
    )
    gate, mult, inlet = (conv[..., k * channels : (k + 1) * channels] for k in range(3))
    product = (mult.astype(F32) * inlet.astype(F32)).astype(BF16)
    taps = conv_taps.shape[0]
    rim = from_behind(product[:, tokens - (taps - 1) :], SP)
    padded = jnp.concatenate([rim, product], axis=1).astype(F32)
    tap_rows = lax.dynamic_slice_in_dim(conv_taps, head * channels, channels, 1)
    mixed = tap_rows[0] * padded[:, :tokens]
    for j in range(1, taps):
        mixed = mixed + tap_rows[j] * padded[:, j : j + tokens]
    conv_out = (gate.astype(F32) * mixed).astype(BF16)
    spans = jnp.arange(tokens)
    causal = spans[:, None] >= spans[None, :]
    pair_logs = jnp.where(
        causal, sums[:, :, None] - sums[:, None, :] + entry[:, None, :], -jnp.inf
    )
    carried_logs = sums + prior_peak
    row_peak = jnp.maximum(carried_logs, jnp.max(pair_logs, axis=-1))
    inner_weights = jnp.exp(pair_logs - row_peak[..., None]) * scale
    carried_weights = jnp.exp(carried_logs - row_peak)
    scores = inner_weights * dot(query, key, (((2,), (2,)), ((0,), (0,))))
    cell = carried_weights[..., None] * dot(query, prior_state, (((2,), (2,)), ((0,), (0,))))
    cell = cell + dot(scores.astype(BF16), value, (((2,), (1,)), ((0,), (0,))))
    cell = cell * lax.rsqrt(jnp.mean(cell * cell, axis=-1, keepdims=True) + EPSILON)
    gain = lax.dynamic_slice_in_dim(head_gain, head * HEAD_DIM, HEAD_DIM, 0)
    mem_out = (cell * gain).astype(BF16)
    both = rolled(jnp.concatenate([conv_out, mem_out], axis=-1), place_x)
    both = exchanged(both, "fs")
    (output,) = call(output_kernel, [((tokens, width), BF16)], [spot], [both, *w_out], 10**9 * 2)

    cores = lax.axis_size("tp")
    parts = exchanged(output.reshape(cores, tokens // cores, width), "tp")
    return jnp.sum(parts.astype(F32), axis=0).astype(BF16)[None]


def solution(mesh):
    sizes = (8, 4, 2, mesh.shape["fs"], mesh.shape["tp"])
    finer = Mesh(mesh.devices.reshape(sizes), (*SP, "fs", "tp"))
    weights = P(SP, ("fs", "tp"))
    return jax.shard_map(
        shards,
        mesh=finer,
        in_specs=(
            P("fs", SP, None),
            P(),
            weights,
            weights,
            weights,
            P(),
            weights,
            weights,
            weights,
            P(),
            P(),
            P(),
            P(None, SP, None),
            P(),
            P(("fs", "tp"), SP),
            P(("fs", "tp"), SP),
        ),
        out_specs=P("fs", SP_TP, None),
        check_vma=False,
    )
```

```python
import jax
import jax.numpy as jnp
from jax import lax
from jax.experimental import pallas as pl
from jax.experimental.pallas import tpu as pltpu
from jax.sharding import Mesh
from jax.sharding import PartitionSpec as P


HEAD_DIM = 128
Y = ("y_hi", "y_lo")
SP = ("z", *Y)
SP_TP = (*SP, "tp")
EPSILON = 1e-06
FAR_BELOW = -1e30
HIGHEST = lax.Precision.HIGHEST
F32 = jnp.float32
BF16 = jnp.bfloat16


def everyone(array, axis):
    copies = jnp.broadcast_to(array, (lax.axis_size(axis), *array.shape))
    return lax.all_to_all(copies, axis, split_axis=0, concat_axis=0, tiled=True)


def exchanged(array, axis):
    return lax.all_to_all(array, axis, split_axis=0, concat_axis=0, tiled=True)


def other_core(array):
    return lax.ppermute(array, "tp", [(0, 1), (1, 0)])


def from_behind(array, axis):
    peers = lax.axis_size(axis)
    return lax.ppermute(array, axis, [(i, i + 1) for i in range(peers - 1)])


def thirds(x):
    first = lax.reduce_precision(x, 8, 7)
    second = lax.reduce_precision(x - first, 8, 7)
    third = lax.reduce_precision(x - first - second, 8, 7)
    return jnp.stack([first, second, third])


def numbers_row(total, peak):
    numbers = thirds(jnp.stack([total, peak])).astype(BF16).reshape(1, -1)
    return jnp.pad(numbers, ((0, 0), (0, HEAD_DIM - numbers.shape[1])))


def numbers_of(rows, seqs):
    found = rows[:, : 6 * seqs].astype(F32).reshape(-1, 3, 2, seqs)
    found = found[:, 0] + found[:, 1] + found[:, 2]
    return found[:, 0].T, found[:, 1].T


def segment_logs(totals, peaks, earlier, after):
    masked = jnp.where(earlier, totals[:, None, :], 0.0)
    dims = (((2,), (0,)), ((), ()))
    between = lax.dot_general(masked, after, dims, precision=HIGHEST)
    logs = jnp.where(earlier, between + peaks[:, None, :], -jnp.inf)
    return jnp.sum(masked, axis=-1), logs


def dot(a, b, dims):
    return lax.dot_general(a, b, dims, preferred_element_type=F32)


def ring(array, axis, by):
    peers = lax.axis_size(axis)
    return lax.ppermute(array, axis, [(i, (i + by) % peers) for i in range(peers)])


def around(array, axis):
    return ring(array, axis, -1), ring(array, axis, 2), ring(array, axis, 1)


def relayed(array, axis):
    cut = array.shape[0] // 2
    ahead = ring(array, axis, -1)
    behind = ring(array, axis, 1)
    first = ring(behind[:cut], axis, 1)
    second = ring(ahead[cut:], axis, -1)
    return ahead, first, second, behind


def rolled(array, by):
    size = array.shape[0]
    twice = jnp.concatenate([array, array], axis=0)
    return lax.dynamic_slice_in_dim(twice, (size - by) % size, size, 0)


def pack_kernel(*refs):
    parts, rest, mem = refs[:8], refs[8], refs[9]
    wide = parts[0].shape[1]
    for k in range(3):
        for copy in range(mem.shape[0]):
            mem[copy, :, k * wide : (k + 1) * wide] = parts[k][...]
    for k in range(5):
        rest[:, k * wide : (k + 1) * wide] = parts[3 + k][...]


def piece(refs, k, other):
    tokens = refs[0].shape[0]
    if k == 0:
        return refs[other][...]
    if other:
        return refs[5][(k - 1) * tokens : k * tokens, :]
    return refs[1 + k][...]


def matmul(core, pieces, weights, k, out):
    half = pieces[0].shape[1]
    first = pl.multiple_of(core * half, half)
    second = pl.multiple_of((1 - core) * half, half)
    wide = out.shape[2]
    mixed = jnp.dot(
        piece(pieces, k, 0), weights[pl.ds(first, half), :wide], preferred_element_type=F32
    )
    mixed += jnp.dot(
        piece(pieces, k, 1), weights[pl.ds(second, half), :wide], preferred_element_type=F32
    )
    out[k] = mixed.astype(BF16)


def project_mem_kernel(spot, bias, *refs):
    parts, pieces, gate_rows, decay = refs[:5], refs[5:11], refs[11], refs[12]
    out, packed, sums_out, entry_out, weights = refs[13:]
    core = spot[0]
    for k, sources in enumerate(((0, 0), (1, 1), (2, 3), (4, 4))):
        place = (spot[2] + k) % 4
        for z in range(8):
            start = pl.multiple_of((z * 4 + place) * 64, 64)
            source = parts[sources[z // 4]]
            row = (z * 64) % source.shape[0]
            weights[pl.ds(start, 64), :] = source[row : row + 64, :]
    dims = (((1,), (1,)), ((), ()))
    gates = [
        dot(gate_rows[core], piece(pieces, k, 0), dims)
        + dot(gate_rows[1 - core], piece(pieces, k, 1), dims)
        for k in range(4)
    ]
    entry = jnp.concatenate([g[0:1] for g in gates], axis=0) + bias[0]
    forget = jnp.concatenate([g[1:2] for g in gates], axis=0) + bias[1]
    small = jnp.exp(-jnp.abs(forget))
    series = small * (1.0 - small * (0.5 - small * (1.0 / 3.0)))
    softened = jnp.where(small < 1e-3, series, jnp.log(1.0 + small))
    log_forget = jnp.minimum(forget, 0.0) - softened + decay[...]
    tokens = entry.shape[1]
    shape = (tokens, tokens)
    upto = lax.broadcasted_iota(jnp.int32, shape, 0) <= lax.broadcasted_iota(jnp.int32, shape, 1)
    sums = jnp.dot(
        log_forget, upto.astype(F32), preferred_element_type=F32, precision=HIGHEST
    )
    sums_out[...] = sums
    entry_out[...] = entry
    total = sums[:, tokens - 1 :]
    local_logs = total - sums + entry
    peak = jnp.max(local_logs, axis=1, keepdims=True)
    local_weights = jnp.exp(local_logs - peak) * HEAD_DIM ** (-0.5)
    columns = jnp.concatenate([local_weights, local_weights], axis=0).T
    for k in range(4):
        matmul(core, pieces, weights, k, out)
        value = out[k, :, 2 * HEAD_DIM :].astype(F32)
        weighted = (value * columns[:, k : k + 1]).astype(BF16)
        state = dot(weighted, out[k, :, HEAD_DIM : 2 * HEAD_DIM], (((0,), (0,)), ((), ())))
        state = state.astype(BF16)
        for c in range(8):
            packed[c, k * 16 : (k + 1) * 16, :] = state[c * 16 : (c + 1) * 16, :]
    numbers = jnp.concatenate([total, peak], axis=0)
    first = numbers.astype(BF16).astype(F32)
    second = (numbers - first).astype(BF16).astype(F32)
    third = numbers - first - second
    numbers = jnp.concatenate([first, second, third, third], axis=0)
    numbers = jnp.broadcast_to(numbers, (32, HEAD_DIM)).astype(BF16)
    for c in range(8):
        packed[c, 64:96, :] = numbers


def project_conv_kernel(spot, *refs):
    for k in range(4):
        matmul(spot[0], refs[:6], refs[6], k, refs[7])


def output_kernel(spot, parts, own, ahead, first, second, behind, out):
    dims = (((1,), (1,)), ((), ()))
    half = first.shape[0]
    for side, far in enumerate((first, second)):
        rows = slice(side * half, (side + 1) * half)
        mixed = dot(parts[spot[1]], own[rows, :], dims)
        mixed += dot(parts[(spot[1] + 1) % 4], ahead[rows, :], dims)
        mixed += dot(parts[(spot[1] + 2) % 4], far[...], dims)
        mixed += dot(parts[(spot[1] + 3) % 4], behind[rows, :], dims)
        out[:, rows] = mixed.astype(BF16)


def in_vmem(count):
    return [pl.BlockSpec(memory_space=pltpu.VMEM)] * count


def call(kernel, shapes, scalars, arrays, flops, scratch=()):
    return pl.pallas_call(
        kernel,
        out_shape=tuple(jax.ShapeDtypeStruct(shape, dtype) for shape, dtype in shapes),
        in_specs=[pl.BlockSpec(memory_space=pltpu.SMEM)] * len(scalars) + in_vmem(len(arrays)),
        out_specs=tuple(in_vmem(len(shapes))),
        scratch_shapes=list(scratch),
        cost_estimate=pl.CostEstimate(flops=flops, bytes_accessed=6 << 20, transcendentals=0),
    )(*scalars, *arrays)


def shards(
    activations,
    norm_gain,
    w_conv_gate,
    w_conv_mult,
    w_conv_in,
    conv_taps,
    w_query,
    w_key,
    w_value,
    w_input_gate,
    w_forget_gate,
    gate_bias,
    decay_shift,
    head_gain,
    w_out_conv,
    w_out_mem,
):
    head = lax.axis_index("fs") * lax.axis_size("tp") + lax.axis_index("tp")
    core = lax.axis_index("tp")
    tokens, width = activations.shape[1:]
    half = width // 2
    seqs = lax.axis_size("fs")

    place_x = lax.axis_index("fs")
    order = [(place_x + by) % seqs for by in range(seqs)]

    place_y = lax.axis_index("y_hi")
    spot = jnp.stack([core, place_x, place_y]).astype(jnp.int32)

    channels = w_conv_gate.shape[1]
    shard = w_query.shape
    pairs = 2 * lax.axis_size("z")
    w_rest, w_mem = call(
        pack_kernel,
        [((shard[0], 5 * shard[1]), BF16), ((pairs, shard[0], 3 * shard[1]), BF16)],
        [],
        [w_query, w_key, w_value, w_conv_gate, w_conv_mult, w_conv_in, w_out_conv.T, w_out_mem.T],
        10**6,
    )
    w_mem = exchanged(w_mem, ("z", "y_lo")).reshape(-1, w_mem.shape[2])
    w_mem = (w_mem, *relayed(w_mem, "y_hi"))

    w_rest = lax.all_gather(w_rest, SP, axis=0, tiled=True)
    w_own = w_rest[:, 3 * channels :]
    w_out = (w_own, *relayed(w_own, "fs"))

    x = activations[0].astype(F32)
    normed = (
        x * lax.rsqrt(jnp.mean(x * x, axis=-1, keepdims=True) + EPSILON) * norm_gain
    ).astype(BF16)
    mine = lax.dynamic_slice_in_dim(normed, core * half, half, 1)
    pieces = [mine, lax.dynamic_slice_in_dim(normed, (1 - core) * half, half, 1)]
    others = around(mine, "fs")
    together = jnp.concatenate(others, axis=0)
    swapped = other_core(together)
    pieces += [*others, swapped]

    gate_rows = jnp.concatenate(
        [
            lax.dynamic_slice_in_dim(w_input_gate, head, 1, 1),
            lax.dynamic_slice_in_dim(w_forget_gate, head, 1, 1),
        ],
        axis=1,
    ).T
    gate_rows = jnp.pad(gate_rows, ((0, 14), (0, 0))).reshape(16, 2, half).transpose(1, 0, 2)
    bias = lax.dynamic_slice_in_dim(gate_bias, head, 1, 1)[:, 0]
    decay = lax.dynamic_slice_in_dim(decay_shift, head, 1, 2)[..., 0]
    decay = jnp.concatenate([lax.dynamic_slice_in_dim(decay, k, 1, 0) for k in order], axis=0)
    places = lax.axis_size(Y)
    cut = HEAD_DIM // places
    qkv, packed, sums, entry = call(
        project_mem_kernel,
        [
            ((seqs, tokens, 3 * HEAD_DIM), BF16),
            ((places, seqs * cut + 32, HEAD_DIM), BF16),
            ((seqs, tokens), F32),
            ((seqs, tokens), F32),
        ],
        [spot, bias],
        [*w_mem, *pieces, gate_rows, decay],
        10**9 * 3,
        [pltpu.VMEM((width, 3 * HEAD_DIM), BF16)],
    )
    query, key, value = (qkv[..., k * HEAD_DIM : (k + 1) * HEAD_DIM] for k in range(3))
    scale = HEAD_DIM ** (-0.5)

    spans = jnp.arange(tokens)
    causal = spans[:, None] >= spans[None, :]
    pair_logs = jnp.where(causal, sums[:, :, None] - sums[:, None, :] + entry[:, None, :], -jnp.inf)
    inner_peak = jnp.max(pair_logs, axis=-1)
    scores = scale * jnp.exp(pair_logs - inner_peak[..., None])
    scores = scores * dot(query, key, (((2,), (2,)), ((0,), (0,))))
    inner = dot(scores.astype(BF16), value, (((2,), (1,)), ((0,), (0,))))
    inner = lax.optimization_barrier(inner)

    packed = exchanged(packed, Y)
    line = jnp.arange(places)
    after = (line[:, None] > line[None, :]).astype(F32)
    totals, peaks = numbers_of(packed[:, seqs * cut :, 0], seqs)
    states = packed[:, : seqs * cut].reshape(places, seqs, cut * HEAD_DIM)
    earlier = jnp.arange(places + 1)[:, None] > line[None, :]
    sums_in, logs = segment_logs(totals, peaks, earlier, after)
    peak_in = jnp.maximum(jnp.max(logs, axis=-1), FAR_BELOW)
    row_mixing = jnp.exp(logs[:, places] - peak_in[:, places, None])
    row_state = jnp.einsum("sj,jsk->sk", row_mixing.astype(BF16), states, preferred_element_type=F32)
    row_numbers = jnp.broadcast_to(
        numbers_row(sums_in[:, places], peak_in[:, places]), (16, HEAD_DIM)
    )
    row_packed = jnp.concatenate(
        [row_state.astype(BF16).reshape(seqs * cut, HEAD_DIM), row_numbers], axis=0
    )
    row_packed = everyone(row_packed, "z")
    row_totals, row_peaks = numbers_of(row_packed[:, seqs * cut], seqs)
    row_states = row_packed[:, : seqs * cut].reshape(places, seqs, cut * HEAD_DIM)
    earlier_rows = (line < lax.axis_index("z"))[None]
    before, row_logs = segment_logs(row_totals, row_peaks, earlier_rows, after)
    start_peak = jnp.maximum(before, jnp.max(row_logs, axis=-1))
    start_mixing = jnp.exp(row_logs - start_peak[..., None])[:, 0]
    start_state = jnp.einsum(
        "sj,jsk->sk", start_mixing.astype(BF16), row_states, preferred_element_type=F32
    )
    moved = sums_in[:, :places] + start_peak
    carried_peak = jnp.maximum(moved, peak_in[:, :places])
    mixing = jnp.exp(logs[:, :places] - carried_peak[..., None]).astype(BF16)
    carried = jnp.einsum("spj,jsk->spk", mixing, states, preferred_element_type=F32)
    carried = carried + jnp.exp(moved - carried_peak)[..., None] * start_state[:, None]
    carried = carried.astype(BF16).transpose(1, 0, 2).reshape(places, seqs * cut, HEAD_DIM)
    carried = exchanged(carried, Y)
    carried = carried.reshape(places, seqs, cut, HEAD_DIM).transpose(1, 0, 2, 3)
    prior_state = carried.reshape(seqs, HEAD_DIM, HEAD_DIM)
    prior_peak = lax.dynamic_slice_in_dim(carried_peak, lax.axis_index(Y), 1, 1)

    (conv,) = call(
        project_conv_kernel,
        [((seqs, tokens, 3 * channels), BF16)],
        [spot],
        [*pieces, w_rest],
        10**9 * 3,
    )
    gate, mult, inlet = (conv[..., k * channels : (k + 1) * channels] for k in range(3))
    product = (mult.astype(F32) * inlet.astype(F32)).astype(BF16)
    taps = conv_taps.shape[0]
    rim = from_behind(product[:, tokens - (taps - 1) :], SP)
    padded = jnp.concatenate([rim, product], axis=1).astype(F32)
    tap_rows = lax.dynamic_slice_in_dim(conv_taps, head * channels, channels, 1)
    mixed = tap_rows[0] * padded[:, :tokens]
    for j in range(1, taps):
        mixed = mixed + tap_rows[j] * padded[:, j : j + tokens]
    conv_out = (gate.astype(F32) * mixed).astype(BF16)
    carried_logs = sums + prior_peak
    row_peak = jnp.maximum(carried_logs, inner_peak)
    inner_scale = jnp.exp(inner_peak - row_peak)
    carried_weights = jnp.exp(carried_logs - row_peak)
    cell = carried_weights[..., None] * dot(query, prior_state, (((2,), (2,)), ((0,), (0,))))
    cell = cell + inner_scale[..., None] * inner
    cell = cell * lax.rsqrt(jnp.mean(cell * cell, axis=-1, keepdims=True) + EPSILON)
    gain = lax.dynamic_slice_in_dim(head_gain, head * HEAD_DIM, HEAD_DIM, 0)
    mem_out = (cell * gain).astype(BF16)
    both = rolled(jnp.concatenate([conv_out, mem_out], axis=-1), place_x)
    both = exchanged(both, "fs")
    (output,) = call(output_kernel, [((tokens, width), BF16)], [spot], [both, *w_out], 10**9 * 2)

    cores = lax.axis_size("tp")
    parts = exchanged(output.reshape(cores, tokens // cores, width), "tp")
    return jnp.sum(parts.astype(F32), axis=0).astype(BF16)[None]


def solution(mesh):
    sizes = (8, 4, 2, mesh.shape["fs"], mesh.shape["tp"])
    finer = Mesh(mesh.devices.reshape(sizes), (*SP, "fs", "tp"))
    weights = P(SP, ("fs", "tp"))
    return jax.shard_map(
        shards,
        mesh=finer,
        in_specs=(
            P("fs", SP, None),
            P(),
            weights,
            weights,
            weights,
            P(),
            weights,
            weights,
            weights,
            P(),
            P(),
            P(),
            P(None, SP, None),
            P(),
            P(("fs", "tp"), SP),
            P(("fs", "tp"), SP),
        ),
        out_specs=P("fs", SP_TP, None),
        check_vma=False,
    )
```
